32 devices in a mesh: sp: 8 (over z, x), tp: 4 (over y, core).
Axes of the slice: x: 2, y: 2, z: 4, core: 2. Of those that a mesh axis runs over, the one named last changes fastest.
Arguments:
- stream: bfloat16 [1024, 2048], P(('sp', 'tp')), may hold values from -2.5 to 2.5
- recurrence_input: bfloat16 [1024, 2, 1024], P('sp', None, 'tp'), may hold values from -6 to 6
- output_gate_input: bfloat16 [1024, 2, 1024], P('sp', None, 'tp'), may hold values from -6 to 6
- convolution_taps: bfloat16 [4, 2, 1024], P(None, None, 'tp'), may hold values from -4 to 4
- first_group_gates: bfloat16 [2, 16, 64, 64], P(None, 'tp'), may hold values from -0.75 to 0.75
- second_group_gates: bfloat16 [2, 8, 128, 128], P(None, 'tp'), may hold values from -0.5 to 0.5
- channel_decay: float32 [2, 1024], P(None, 'tp'), may hold values from 4.7 to 13.6
- position_log_extra: float32 [1024, 2, 1024], P('sp', None, 'tp'), may hold values from -1.4 to 0, as said below
- recurrence_output_weight: bfloat16 [2, 1024, 2048], P(None, 'tp'), may hold values from -0.125 to 0.125
- first_norm_gain: float32 [2048], replicated, may hold values from 0.1 to 1.9
- first_norm_bias: float32 [2048], replicated, may hold values from -1.75 to 1.75
- routed_expert_index: int32 [1024, 4], P('sp'), may hold values from 0 to 7, all different within a row; in each aligned block of 32 rows (0 to 31, 32 to 63, ...) at most 20 rows name the same one
- routed_expert_weight: float32 [1024, 4], P('sp'), may hold values from 0.25 to 1
- routed_gate_weight: bfloat16 [8, 2048, 512], P('sp', None, 'tp'), may hold values from -0.125 to 0.125
- routed_up_weight: bfloat16 [8, 2048, 512], P('sp', None, 'tp'), may hold values from -0.125 to 0.125
- routed_down_weight: bfloat16 [8, 512, 2048], P('sp', 'tp'), may hold values from -0.25 to 0.25
- shared_gate_weight: bfloat16 [2048, 512], replicated, may hold values from -0.125 to 0.125
- shared_up_weight: bfloat16 [2048, 512], replicated, may hold values from -0.125 to 0.125
- shared_down_weight: bfloat16 [512, 2048], replicated, may hold values from -0.25 to 0.25
- second_norm_gain: float32 [2048], replicated, may hold values from 0.1 to 1.9
- second_norm_bias: float32 [2048], replicated, may hold values from -1.75 to 1.75
Outputs:
- result: bfloat16 [1024, 2048], P(('sp', 'tp'))
The draws below stay inside these ranges and needn't reach their ends.
Inputs may be any that keep to these rules, and one draw needn't show every extreme that they name: `routed_expert_index`: each row names 4 different experts. In each aligned block of 32 rows no expert is named more than 20 times, and in some block an expert is named exactly 20 times. `position_log_extra`: every entry is negative.
All inputs are finite; a program needn't handle non-finite values.
Results may differ from the reference program's by a relative error of at most 0.015.
Values may be sent and summed in bfloat16 or wider, within the bound.
A program may use at most 64 MiB of HBM per device.

```python
import math
import jax
import jax.numpy as jnp
import numpy as np
from jax import lax

D = 2048
D_HALF = 1024
HEAD_SMALL = 64
HEAD_LARGE = 128
HEADS_SMALL = 16
HEADS_LARGE = 8
DQ = 256
CONV = 4
FE = 512
FE_DEV = 128
FS = 512
K = 4
EXPERTS = 8
TOK_DEV = 128
TOK_Q = 32
TOKENS = 1024
CAP_Q = 20
N_TP = 4


def draw_channel_decay(key, part):
    key_flag = jax.random.fold_in(key, 11)
    key_rate = jax.random.fold_in(key, 12)
    fast_limit = 5
    flags = jax.random.randint(key_flag, (2, D_HALF // HEAD_SMALL), 0, 10) < fast_limit
    channel = jnp.arange(D_HALF)
    head_index = jnp.stack([channel // HEAD_SMALL, channel // HEAD_LARGE])
    fast = jnp.take_along_axis(flags, head_index, axis=1)
    spread = jax.random.uniform(key_rate, (2, D_HALF), jnp.float32)
    fast_rate = jnp.exp(jnp.log(0.005) + spread * jnp.log(0.009 / 0.005))
    slow_rate = jnp.exp(jnp.log(1.25e-06) + spread * jnp.log(4.0))
    rate = jnp.where(fast, fast_rate, slow_rate)
    return -jnp.log(jnp.expm1(rate))


def draw_position_log_extra(key, part):
    key_base = jax.random.fold_in(key, 21)
    key_spot = jax.random.fold_in(key, 22)
    key_depth = jax.random.fold_in(key, 23)
    block_count = TOKENS // TOK_DEV
    base = jnp.exp(jax.random.uniform(key_base, (block_count, 1, 2, D_HALF), jnp.float32, jnp.log(5e-06), jnp.log(2e-05)))
    base = jnp.broadcast_to(base, (block_count, TOK_DEV, 2, D_HALF)).reshape(TOKENS, 2, D_HALF)
    spots = jax.random.randint(key_spot, (2,), 0, TOKENS)
    position = jnp.arange(TOKENS)
    hits = jnp.sum((position[:, None] == spots[None, :]).astype(jnp.float32), axis=1)
    depth = jax.random.uniform(key_depth, (2, D_HALF), jnp.float32, 0.22, 0.69)
    return -(base + hits[:, None, None] * depth[None])


def levels(own_key, shape, split, low, top_value):
    level, own = 1.0, jax.random.fold_in(own_key, 6)
    for dim, parts in split:
        heights = jnp.exp(jax.random.uniform(jax.random.fold_in(own, dim), (parts,), jnp.float32, low / len(split), top_value / len(split)))
        level = level * jnp.repeat(heights, shape[dim] // parts).reshape([-1 if axis == dim else 1 for axis in range(len(shape))])
    return level


def deal_out(rng, own, number, rows, count, top, limit, slope):
    sequence = jax.random.permutation(rng, count)
    heavy_load, ordinary = portions_of(count, rows * top, limit, slope, True), portions_of(count, rows * top, limit, slope, False)
    places = jnp.arange(count)

    def named(tallies, rotation):
        used = int((tallies > 0).sum())
        fixed = max(1, used // 4)
        moved = fixed + (places - fixed + rotation * (used - fixed)) % max(1, count - fixed)
        return jnp.zeros((count,), jnp.int32).at[sequence[jnp.where(places < fixed, places, moved)]].set(jnp.asarray(tallies, jnp.int32))

    tallies = jnp.where(number % 4 == 0, named(heavy_load, number // 4), named(ordinary, number - number // 4 - 1))
    mixed = jax.random.permutation(jax.random.fold_in(own, 3), count)
    donor, sink = mixed[0:count // 2 * 2:2], mixed[1:count // 2 * 2:2]
    margin = jnp.minimum(tallies[donor] - 1, limit - tallies[sink]) // 2
    margin = jnp.where((donor == sequence[0]) | (sink == sequence[0]) | (tallies[sink] == 0), 0, jnp.maximum(margin, 0))
    moved = jax.random.randint(jax.random.fold_in(own, 4), (count // 2,), 0, 1 << 20) % (margin + 1)
    tallies = tallies.at[donor].add(-moved).at[sink].add(moved)
    items = jnp.searchsorted(jnp.cumsum(tallies), jnp.arange(rows * top), side="right").astype(jnp.int32)
    table = items.reshape(top, rows).T
    table = table[jax.random.permutation(jax.random.fold_in(own, 1), rows)]
    rotation = jax.random.randint(jax.random.fold_in(own, 2), (rows, 1), 0, top)
    return jnp.take_along_axis(table, (jnp.arange(top)[None, :] + rotation) % top, axis=1)


def portions_of(number_of, total, reach, skew, full):
    portions = [(1 << 20) // math.isqrt(grade ** skew) + 1 for grade in range(1, number_of + 1)]
    largest = reach if full else min(reach, max(-(-total // number_of), total * portions[0] // sum(portions)))
    least = 1 if total - largest >= number_of - 1 else 0
    counts, spare = [largest] + [least] * (number_of - 1), total - largest - least * (number_of - 1)
    while spare > 0:
        movable = [i for i in range(1, number_of) if counts[i] < largest] or [i for i in range(1, number_of) if counts[i] < reach]
        mass, budget = sum([portions[i] for i in movable]), spare
        for i in movable:
            more = min(reach - counts[i], max(1, budget * portions[i] // mass), spare)
            counts[i] = counts[i] + more
            spare = spare - more
    return np.array(counts)


def noise(key, dims, scale, most, pieces=(), held_as=jnp.bfloat16):
    array = jax.random.normal(key, dims, jnp.float32) * scale
    if len(pieces) > 0:
        array = levels(key, dims, pieces, -0.22, 0.18) * array
    return jnp.clip(array, min=-most, max=most).astype(held_as)


def setup_inputs(seed: int = 0) -> dict:
    streams_of = jax.random.split(jax.random.key(seed), 22)
    stream = noise(streams_of[0], (TOKENS, D), 0.4, 2.5, ((0, 32),))
    recurrence_input = noise(streams_of[1], (TOKENS, 2, D_HALF), 1.0, 6.0, ((0, 8), (2, 4)))
    output_gate_input = noise(streams_of[2], (TOKENS, 2, D_HALF), 1.0, 6.0, ((0, 8), (2, 4)))
    convolution_taps = noise(streams_of[3], (CONV, 2, D_HALF), 1.0, 4.0, ((2, 4),))
    first_group_gates = noise(streams_of[4], (2, HEADS_SMALL, HEAD_SMALL, HEAD_SMALL), HEAD_SMALL ** -0.5, 0.75, ((1, 4),))
    second_group_gates = noise(streams_of[5], (2, HEADS_LARGE, HEAD_LARGE, HEAD_LARGE), HEAD_LARGE ** -0.5, 0.5, ((1, 4),))
    channel_decay = draw_channel_decay(jax.random.fold_in(streams_of[21], 71), 0)
    position_log_extra = draw_position_log_extra(jax.random.fold_in(streams_of[21], 71), 0)
    recurrence_output_weight = noise(streams_of[8], (2, D_HALF, D), (2 * D_HALF) ** -0.5, 0.125, ((1, 4),))
    first_norm_gain = jnp.clip(1.0 + 0.18 * jax.random.normal(streams_of[9], (D,), jnp.float32), 0.1, 1.9)
    first_norm_bias = noise(streams_of[10], (D,), 0.3, 1.75, (), jnp.float32)
    routed_expert_index_keys = jax.random.split(jax.random.fold_in(streams_of[11], 1), TOKENS // TOK_Q)
    routed_expert_index_turns = jax.random.permutation(jax.random.fold_in(streams_of[11], 3), TOKENS // TOK_Q)
    routed_expert_index = jax.vmap(lambda own, number: deal_out(jax.random.fold_in(streams_of[11], 2), own, number, TOK_Q, EXPERTS, K, CAP_Q, 1))(routed_expert_index_keys, routed_expert_index_turns).reshape((TOKENS, K))
    routed_expert_weight = jnp.clip(0.25 + 0.75 * jax.random.uniform(streams_of[12], (TOKENS, K), jnp.float32) ** levels(streams_of[12], (TOKENS, K), ((0, 8),), -0.2, 0.2), 0.25, 1.0)
    routed_gate_weight = noise(streams_of[13], (EXPERTS, D, FE), D ** -0.5, 0.125, ((0, 8), (2, 4)))
    routed_up_weight = noise(streams_of[14], (EXPERTS, D, FE), D ** -0.5, 0.125, ((0, 8), (2, 4)))
    routed_down_weight = noise(streams_of[15], (EXPERTS, FE, D), FE ** -0.5, 0.25, ((0, 8), (1, 4)))
    shared_gate_weight = noise(streams_of[16], (D, FS), D ** -0.5, 0.125)
    shared_up_weight = noise(streams_of[17], (D, FS), D ** -0.5, 0.125)
    shared_down_weight = noise(streams_of[18], (FS, D), FS ** -0.5, 0.25)
    second_norm_gain = jnp.clip(1.0 + 0.18 * jax.random.normal(streams_of[19], (D,), jnp.float32), 0.1, 1.9)
    second_norm_bias = noise(streams_of[20], (D,), 0.3, 1.75, (), jnp.float32)
    return {"stream": stream, "recurrence_input": recurrence_input, "output_gate_input": output_gate_input, "convolution_taps": convolution_taps, "first_group_gates": first_group_gates, "second_group_gates": second_group_gates, "channel_decay": channel_decay, "position_log_extra": position_log_extra, "recurrence_output_weight": recurrence_output_weight, "first_norm_gain": first_norm_gain, "first_norm_bias": first_norm_bias, "routed_expert_index": routed_expert_index, "routed_expert_weight": routed_expert_weight, "routed_gate_weight": routed_gate_weight, "routed_up_weight": routed_up_weight, "routed_down_weight": routed_down_weight, "shared_gate_weight": shared_gate_weight, "shared_up_weight": shared_up_weight, "shared_down_weight": shared_down_weight, "second_norm_gain": second_norm_gain, "second_norm_bias": second_norm_bias}


RESIDUAL_SCALE = 8.0 ** 0.25
NORM_EPSILON = 1e-05

def layer_norm(values, gain_vec, bias_vec):
    row_mean = lax.optimization_barrier(jnp.mean(values, axis=-1, keepdims=True))
    spread = lax.optimization_barrier(jnp.mean(jnp.square(values - row_mean), axis=-1, keepdims=True))
    return (values - row_mean) * lax.rsqrt(spread + NORM_EPSILON) * gain_vec + bias_vec

def rounded(values):
    return lax.optimization_barrier(values.astype(jnp.bfloat16)).astype(jnp.float32)

def block_gates(conv_rows, weights, head_size):
    length = conv_rows.shape[0]
    head_rows = conv_rows.reshape(length, -1, head_size).astype(jnp.float32)
    pre_act = jnp.einsum('thc,ghcd->gthd', head_rows, weights.astype(jnp.float32))
    gate_pair = jax.nn.sigmoid(pre_act).reshape(2, length, -1)
    return (gate_pair[0], gate_pair[1])

def chain_link(first_part, second_part):
    return (first_part[0] * second_part[0], second_part[0] * first_part[1] + second_part[1])

def recurrence_result(recurrence_input, output_gate_input, convolution_taps, first_group_gates, second_group_gates, channel_decay, position_log_extra):
    length = recurrence_input.shape[0]
    tap_count = convolution_taps.shape[0]
    padded = jnp.pad(recurrence_input.astype(jnp.float32), ((tap_count - 1, 0), (0, 0), (0, 0)))
    tap_weights = convolution_taps.astype(jnp.float32)
    summed = tap_weights[0] * padded[0:length]
    for offset in range(1, tap_count):
        summed = summed + tap_weights[offset] * padded[offset:offset + length]
    conv_rows = summed.astype(jnp.bfloat16)
    recur_a, input_a = block_gates(conv_rows[:, 0], first_group_gates, first_group_gates.shape[-1])
    recur_b, input_b = block_gates(conv_rows[:, 1], second_group_gates, second_group_gates.shape[-1])
    recurrence_gate = jnp.stack([recur_a, recur_b], axis=1)
    input_gate = jnp.stack([input_a, input_b], axis=1)
    decay_logarithm = -8.0 * recurrence_gate * jax.nn.softplus(-channel_decay) + position_log_extra
    driving = jnp.sqrt(-jnp.expm1(2.0 * decay_logarithm)) * input_gate * conv_rows.astype(jnp.float32)
    states = lax.associative_scan(chain_link, (jnp.exp(decay_logarithm), driving), axis=0)[1]
    return (jax.nn.gelu(output_gate_input.astype(jnp.float32)) * states).astype(jnp.bfloat16)

def reference(stream, recurrence_input, output_gate_input, convolution_taps, first_group_gates, second_group_gates, channel_decay, position_log_extra, recurrence_output_weight, first_norm_gain, first_norm_bias, routed_expert_index, routed_expert_weight, routed_gate_weight, routed_up_weight, routed_down_weight, shared_gate_weight, shared_up_weight, shared_down_weight, second_norm_gain, second_norm_bias):
    branch_output = recurrence_result(recurrence_input, output_gate_input, convolution_taps, first_group_gates, second_group_gates, channel_decay, position_log_extra)
    run_rows = branch_output.reshape(TOKENS, 2, N_TP, DQ)
    run_weights = recurrence_output_weight.reshape(2, N_TP, DQ, D)
    mixed = jnp.zeros((TOKENS, D), jnp.float32)
    for run_index in range(N_TP):
        partial_value = jnp.einsum('tgc,gcd->td', run_rows[:, :, run_index].astype(jnp.float32), run_weights[:, run_index].astype(jnp.float32))
        mixed = mixed + rounded(partial_value)
    normed = layer_norm(RESIDUAL_SCALE * stream.astype(jnp.float32) + mixed, first_norm_gain, first_norm_bias).astype(jnp.bfloat16)
    block_count = TOKENS // TOK_Q
    block_ids = routed_expert_index.reshape(block_count, TOK_Q * K)
    onehot = (block_ids[:, :, None] == jnp.arange(EXPERTS, dtype=jnp.int32)[None, None, :]).astype(jnp.int32)
    slot_ranks = lax.optimization_barrier(jnp.sum((jnp.cumsum(onehot, axis=1) - onehot) * onehot, axis=2)).astype(jnp.int32)
    targets = (block_ids * block_count + jnp.arange(block_count, dtype=jnp.int32)[:, None]) * CAP_Q + slot_ranks
    entries = jnp.arange(TOKENS * K, dtype=jnp.int32).reshape(block_count, TOK_Q * K)
    table = jnp.full((EXPERTS * block_count * CAP_Q,), TOKENS * K, jnp.int32)
    table = table.at[targets.reshape(-1)].set(entries.reshape(-1)).reshape(EXPERTS, block_count * CAP_Q)
    padded_rows = jnp.concatenate([normed, jnp.zeros((1, D), jnp.bfloat16)], axis=0)
    padded_weights = jnp.concatenate([routed_expert_weight.reshape(-1), jnp.zeros((1,), jnp.float32)])

    def expert_step(routed, inputs):
        entry_rows, gate_w, up_w, down_w = inputs
        token_rows = entry_rows // K
        picked = padded_rows[token_rows]
        hidden = (jax.nn.silu(jnp.dot(picked, gate_w, preferred_element_type=jnp.float32)) * jnp.dot(picked, up_w, preferred_element_type=jnp.float32)).astype(jnp.bfloat16)
        summed_out = jnp.zeros((picked.shape[0], D), jnp.float32)
        for run_index in range(N_TP):
            partial_out = jnp.dot(hidden[:, run_index * FE_DEV:(run_index + 1) * FE_DEV], down_w[run_index * FE_DEV:(run_index + 1) * FE_DEV], preferred_element_type=jnp.float32)
            summed_out = summed_out + rounded(partial_out)
        weighted = padded_weights[entry_rows][:, None] * rounded(summed_out)
        return (routed.at[token_rows].add(weighted), None)
    routed = lax.scan(expert_step, jnp.zeros((TOKENS + 1, D), jnp.float32), (table, routed_gate_weight, routed_up_weight, routed_down_weight))[0][:TOKENS]
    shared_hidden = (jax.nn.silu(jnp.dot(normed, shared_gate_weight, preferred_element_type=jnp.float32)) * jnp.dot(normed, shared_up_weight, preferred_element_type=jnp.float32)).astype(jnp.bfloat16)
    shared_out = jnp.dot(shared_hidden, shared_down_weight, preferred_element_type=jnp.float32)
    moe = shared_out + routed
    final = layer_norm(RESIDUAL_SCALE * normed.astype(jnp.float32) + moe, second_norm_gain, second_norm_bias)
    return final.astype(jnp.bfloat16)
```

```python
import functools

import jax
import jax.numpy as jnp
from jax import lax
from jax.experimental import pallas as pl
from jax.experimental.pallas import tpu as pltpu
from jax.sharding import PartitionSpec as P

RESIDUAL_SCALE = 8.0**0.25
NORM_EPSILON = 1e-05
LANES = 128
PIECES = 6
EARLY = 3
MESH = pl.DeviceIdType.MESH
F32 = jnp.float32
BF16 = jnp.bfloat16


def layer_norm(values, gain, bias):
    row_mean = jnp.mean(values, axis=-1, keepdims=True)
    spread = jnp.mean(jnp.square(values - row_mean), axis=-1, keepdims=True)
    return (values - row_mean) * lax.rsqrt(spread + NORM_EPSILON) * gain + bias


def expm1_negative(z):
    small = jnp.full_like(z, 1.0 / 40320.0)
    for n in (5040.0, 720.0, 120.0, 24.0, 6.0, 2.0, 1.0):
        small = small * z + 1.0 / n
    return jnp.where(z > -0.5, small * z, jnp.exp(z) - 1.0)


def softplus(y):
    u = jnp.exp(-jnp.abs(y))
    s = u / (2.0 + u)
    sq = s * s
    series = jnp.full_like(s, 1.0 / 17.0)
    for n in (15.0, 13.0, 11.0, 9.0, 7.0, 5.0, 3.0, 1.0):
        series = series * sq + 1.0 / n
    return jnp.maximum(y, 0.0) + 2.0 * s * series


def lane_blocks(maps_ref):
    kinds, heads, size, _ = maps_ref.shape
    per = LANES // size
    blocks = []
    for start in range(0, heads, per):
        sides = []
        for kind in range(kinds):
            if per == 1:
                sides.append(maps_ref[kind, start])
                continue
            tall = []
            for p in range(per):
                row = lax.broadcasted_iota(jnp.int32, (size, LANES), 0)
                col = lax.broadcasted_iota(jnp.int32, (size, LANES), 1)
                place = jnp.where(col == row + p * size, 1.0, 0.0).astype(BF16)
                tall.append(dot(maps_ref[kind, start + p], place))
            sides.append(jnp.concatenate(tall, axis=0).astype(BF16))
        blocks.append(jnp.concatenate(sides, axis=1))
    return blocks


def silu(v):
    return v * jax.nn.sigmoid(v)


def dot(a, b):
    return jnp.dot(a, b, preferred_element_type=F32)


def kernel(
    dims,
    stream_hbm, rec_hbm, gate_hbm, taps_hbm, small_hbm, large_hbm, decay_hbm, extra_hbm,
    n1g_hbm, n1b_hbm, n2g_hbm, n2b_hbm, ids_hbm, wts_hbm,
    out_w_hbm, rg_hbm, ru_hbm, rd_hbm, sg_hbm, su_hbm, sd_hbm,
    result,
    stream, rec_in, gate_in, taps, small_maps, large_maps, channel_decay, extra, n1g, n1b, n2g, n2b,
    ids, wts, in_sem,
    padded, halo, carry_own, carry_in, wdense, w_in, out_w, w_gu, w_d, s_gu, s_d,
    part, part_in, rows, hid, y_part, x_in, z_out, z_in, moe,
    local_sem, halo_sem, carry_send, carry_recv, w_send, w_recv,
    wt_send, wt_recv, tp_send, tp_recv, ag_send, ag_recv, fw_send, fw_recv,
    xs_send, xs_recv, zs_send, zs_recv,
):
    sp_n, tp_n, inner = dims
    outer = sp_n // inner
    pairs = tp_n // 2
    sp, tp = lax.axis_index("sp"), lax.axis_index("tp")
    zi, xi = sp // inner, lax.rem(sp, inner)
    other_x = lax.rem(xi + 1, inner)
    x_peer = zi * inner + other_x
    half_c = lax.rem(tp, 2)
    yi = tp // 2
    mate = yi * 2 + (1 - half_c)
    length = rec_in.shape[0]
    chans = rec_in.shape[1] * rec_in.shape[2]
    quarter = stream.shape[0]
    fe = rg_hbm.shape[1]
    fs = sg_hbm.shape[1]

    loads = [
        pltpu.make_async_copy(src, dst, in_sem.at[i])
        for i, (src, dst) in enumerate([
            (rec_hbm, rec_in), (small_hbm, small_maps), (large_hbm, large_maps), (taps_hbm, taps),
            (decay_hbm, channel_decay), (extra_hbm, extra), (gate_hbm, gate_in), (ids_hbm, ids),
            (wts_hbm, wts), (stream_hbm, stream), (n1g_hbm, n1g), (n1b_hbm, n1b), (n2g_hbm, n2g),
            (n2b_hbm, n2b),
        ])
    ]
    for load in loads:
        load.start()
    barrier = pltpu.get_barrier_semaphore()

    @pl.loop(1, sp_n)
    def _(step):
        pl.semaphore_signal(
            barrier, inc=1, device_id=(lax.rem(sp + step, sp_n), tp), device_id_type=MESH
        )

    for step in range(1, tp_n):
        pl.semaphore_signal(
            barrier, inc=1, device_id=(sp, lax.rem(tp + step, tp_n)), device_id_type=MESH
        )
    for load in loads:
        load.wait()
    pl.semaphore_wait(barrier, sp_n - 1 + tp_n - 1)

    def remote(src, dst, send, recv, where):
        return pltpu.make_async_remote_copy(
            src_ref=src, dst_ref=dst, send_sem=send, recv_sem=recv,
            device_id=where, device_id_type=MESH,
        )

    locals_ = [
        pltpu.make_async_copy(rg_hbm, w_gu.at[tp, :, pl.ds(0, fe)], local_sem.at[0]),
        pltpu.make_async_copy(ru_hbm, w_gu.at[tp, :, pl.ds(fe, fe)], local_sem.at[1]),
        pltpu.make_async_copy(rd_hbm, w_d.at[tp], local_sem.at[2]),
        pltpu.make_async_copy(out_w_hbm, out_w, local_sem.at[3]),
        pltpu.make_async_copy(sg_hbm, s_gu.at[:, pl.ds(0, fs)], local_sem.at[4]),
        pltpu.make_async_copy(su_hbm, s_gu.at[:, pl.ds(fs, fs)], local_sem.at[5]),
        pltpu.make_async_copy(sd_hbm, s_d, local_sem.at[6]),
    ]

    halo_copy = remote(
        rec_in.at[pl.ds(length - 8, 8)], halo, halo_sem.at[0], halo_sem.at[1],
        (lax.rem(sp + 1, sp_n), tp),
    )

    @pl.when(sp + 1 < sp_n)
    def _():
        halo_copy.start()

    depth = rg_hbm.shape[0] // 2
    fe_half = fe // 2

    def weight_src(piece):
        kind, part_id = piece // 2, piece % 2
        if kind == 2:
            return rd_hbm.at[pl.ds(part_id * fe_half, fe_half)]
        return (rg_hbm, ru_hbm)[kind].at[pl.ds(part_id * depth, depth)]

    def weight_dst(slot, piece):
        kind, part_id = piece // 2, piece % 2
        if kind == 2:
            return w_d.at[slot, pl.ds(part_id * fe_half, fe_half)]
        return w_gu.at[slot, pl.ds(part_id * depth, depth), pl.ds(kind * fe, fe)]

    def weight_out(kind, step):
        return remote(
            weight_src(kind), weight_dst(tp, kind),
            wt_send.at[kind, step], wt_recv.at[kind, tp],
            (sp, lax.rem(yi + step, pairs) * 2 + half_c),
        )

    def weight_mate(kind, slot, step):
        src = weight_src(kind) if step == 0 else weight_dst(slot, kind)
        return remote(
            src, weight_dst(slot, kind),
            wt_send.at[kind, pairs + step], wt_recv.at[kind, slot], (sp, mate),
        )

    def pair_slot(step):
        return lax.rem(yi + step, pairs) * 2 + half_c

    for piece in range(EARLY):
        for step in range(1, pairs):
            weight_out(piece, step).start()
    locals_[3].start()
    for piece in range(PIECES):
        weight_mate(piece, tp, 0).start()
    for i in range(3):
        locals_[i].start()
    for i in (4, 5, 6):
        locals_[i].start()

    expert = lax.broadcasted_iota(jnp.int32, (wdense.shape[0], length), 0)
    table = jnp.zeros((wdense.shape[0], length), F32)
    for k in range(ids.shape[0]):
        table = table + jnp.where(expert == ids[k : k + 1], wts[k : k + 1], 0.0)
    wdense[...] = table
    w_in[sp] = table

    def w_out(step):
        return remote(
            wdense, w_in.at[sp], w_send.at[step], w_recv.at[sp], (lax.rem(sp + step, sp_n), tp)
        )

    @pl.loop(1, sp_n)
    def _(step):
        w_out(step).start()

    small_blocks, large_blocks = lane_blocks(small_maps), lane_blocks(large_maps)
    rate_rows = -8.0 * softplus(-channel_decay[...])
    rate = jnp.concatenate([rate_rows[0:1], rate_rows[1:2]], axis=1)
    tap_rows = [
        jnp.concatenate([taps[k, 0:1], taps[k, 1:2]], axis=1).astype(F32)
        for k in range(taps.shape[0])
    ]

    padded[pl.ds(8, length)] = rec_in[...].astype(F32).reshape(length, chans)

    @pl.when(sp == 0)
    def _():
        padded[pl.ds(0, 8)] = jnp.zeros((8, chans), F32)

    @pl.when(sp > 0)
    def _():
        halo_copy.wait_recv()
        padded[pl.ds(0, 8)] = halo[...].astype(F32).reshape(8, chans)

    tap_n = taps.shape[0]
    summed = tap_rows[0] * padded[pl.ds(8 - tap_n + 1, length)]
    for k in range(1, tap_n):
        summed = summed + tap_rows[k] * padded[pl.ds(8 - tap_n + 1 + k, length)]
    conv = summed.astype(BF16)
    outs = [
        dot(conv[:, i * LANES : (i + 1) * LANES], maps)
        for i, maps in enumerate(small_blocks + large_blocks)
    ]
    recur = jax.nn.sigmoid(jnp.concatenate([o[:, :LANES] for o in outs], axis=1))
    inp = jax.nn.sigmoid(jnp.concatenate([o[:, LANES:] for o in outs], axis=1))
    log_decay = recur * rate + extra[...].reshape(length, chans)
    decay = jnp.exp(log_decay)
    state = jnp.sqrt(-expm1_negative(2.0 * log_decay)) * inp * conv.astype(F32)
    row_id = lax.broadcasted_iota(jnp.int32, (length, chans), 0)
    shift = 1
    while shift < length:
        live = row_id >= shift
        before_a = jnp.where(live, pltpu.roll(decay, shift, 0), 1.0)
        before_b = jnp.where(live, pltpu.roll(state, shift, 0), 0.0)
        state = decay * before_b + state
        decay = decay * before_a
        shift *= 2
    carry_own[...] = jnp.concatenate(
        [decay[length - 1 :], state[length - 1 :]], axis=0
    )

    def carry_out(step):
        return remote(
            carry_own, carry_in.at[sp], carry_send.at[step], carry_recv.at[sp],
            (lax.rem(sp + step, sp_n), tp),
        )

    def carry_arrival(who):
        return remote(
            carry_own, carry_in.at[who], carry_send.at[0], carry_recv.at[who], (sp, tp)
        )

    @pl.loop(1, sp_n)
    def _(step):
        @pl.when(sp + step < sp_n)
        def _():
            carry_out(step).start()

    gi = gate_in[...].astype(F32).reshape(length, chans)
    gelu = 0.5 * gi * (1.0 + jnp.tanh(0.7978845608028654 * (gi + 0.044715 * gi * gi * gi)))

    def fold(who, incoming):
        carry_arrival(who).wait_recv()
        link = carry_in[who]
        return link[0:1] * incoming + link[1:2]

    incoming = lax.fori_loop(0, sp, fold, jnp.zeros((1, chans), F32))
    branch = (gelu * (state + decay * incoming)).astype(BF16)
    locals_[3].wait()
    part[...] = dot(branch, out_w[...]).astype(BF16).reshape(part.shape)

    def part_out(step):
        to = lax.rem(tp + step, tp_n)
        return remote(
            part.at[to], part_in.at[tp], tp_send.at[step], tp_recv.at[tp], (sp, to)
        )

    def part_arrival(who):
        return remote(part.at[who], part_in.at[who], tp_send.at[0], tp_recv.at[who], (sp, tp))

    for step in range(1, tp_n):
        part_out(step).start()
    for piece in range(EARLY, PIECES):
        for step in range(1, pairs):
            weight_out(piece, step).start()
    mixed = part[tp].astype(F32)
    for step in range(1, tp_n):
        who = lax.rem(tp + step, tp_n)
        part_arrival(who).wait_recv()
        mixed = mixed + part_in[who].astype(F32)
    normed = layer_norm(
        RESIDUAL_SCALE * stream[...].astype(F32) + mixed, n1g[...], n1b[...]
    ).astype(BF16)
    rows[sp] = normed

    def ag_out(step):
        return remote(
            rows.at[sp], rows.at[sp], ag_send.at[step], ag_recv.at[sp],
            (lax.rem(zi + step, outer) * inner + xi, tp),
        )

    def ag_arrival(who):
        return remote(rows.at[who], rows.at[who], ag_send.at[0], ag_recv.at[who], (sp, tp))

    def forward(who):
        return remote(
            rows.at[who], rows.at[who], fw_send.at[who], ag_recv.at[who], (x_peer, tp)
        )

    @pl.loop(1, outer)
    def _(step):
        ag_out(step).start()

    forward(sp).start()

    def weight_arrival(kind, slot):
        return remote(
            weight_dst(slot, kind), weight_dst(slot, kind),
            wt_send.at[kind, 0], wt_recv.at[kind, slot], (sp, mate),
        )

    def relay(piece):
        for step in range(1, pairs):
            weight_arrival(piece, pair_slot(step)).wait_recv()
            weight_mate(piece, pair_slot(step), step).start()

    for piece in range(EARLY):
        relay(piece)

    locals_[4].wait()
    locals_[5].wait()
    locals_[6].wait()
    up = dot(normed, s_gu[...])
    s_hid = (silu(up[:, :fs]) * up[:, fs:]).astype(BF16)
    moe[...] = dot(s_hid, s_d[...]) + RESIDUAL_SCALE * normed.astype(F32)

    @pl.loop(1, sp_n)
    def _(step):
        who = lax.rem(sp + step, sp_n)
        remote(wdense, w_in.at[who], w_send.at[0], w_recv.at[who], (sp, tp)).wait_recv()

    for i in range(3):
        locals_[i].wait()

    @pl.loop(1, outer)
    def _(step):
        mine = lax.rem(zi + step, outer) * inner + xi
        ag_arrival(mine).wait_recv()
        forward(mine).start()

    for piece in range(EARLY, PIECES):
        relay(piece)

    @pl.loop(0, outer)
    def _(step):
        ag_arrival(step * inner + other_x).wait_recv()

    for piece in range(PIECES):
        for step in range(pairs):
            weight_arrival(piece, lax.rem(yi + step, pairs) * 2 + 1 - half_c).wait_recv()

    width = stream.shape[1]
    grp = inner * quarter
    batch = min(sp_n, 8)

    @pl.loop(0, sp_n // batch)
    def _(i):
        block = rows[pl.ds(i * batch, batch)].reshape(batch * quarter, width)
        for t in range(tp_n):
            gu = dot(block, w_gu[t])
            act = (silu(gu[:, :fe]) * gu[:, fe:]).astype(BF16)
            hid[pl.ds(i * batch, batch), :, t * fe : (t + 1) * fe] = act.reshape(
                batch, quarter, fe
            )

    def x_out(zj):
        return remote(
            y_part.at[zj * inner + other_x], x_in.at[zj], xs_send.at[zj], xs_recv.at[zj],
            (x_peer, tp),
        )

    own_rows = lax.broadcasted_iota(jnp.int32, (quarter, length), 0) + tp * quarter
    pick = lax.broadcasted_iota(jnp.int32, (quarter, length), 1) == own_rows

    @pl.loop(1, outer + 1)
    def _(step):
        zj = lax.rem(zi + step, outer)
        block = hid[pl.ds(zj * inner, inner)].reshape(grp, tp_n * fe)
        value = dot(block, w_d[...].reshape(tp_n * fe, width))
        for j in range(inner):
            line = w_in[zj * inner + j, pl.ds(sp, 1)]
            weight = jnp.sum(jnp.where(pick, line, 0.0), axis=1, keepdims=True)
            y_part[zj * inner + j] = (
                weight * value[j * quarter : (j + 1) * quarter]
            ).astype(BF16)
        x_out(zj).start()

    def z_send(step):
        zj = lax.rem(zi + step, outer)
        return remote(
            z_out.at[zj], z_in.at[zi], zs_send.at[step], zs_recv.at[zi], (zj * inner + xi, tp)
        )

    @pl.loop(1, outer)
    def _(step):
        zj = lax.rem(zi + step, outer)
        x_out(zj).wait_recv()
        both = y_part[zj * inner + xi].astype(F32) + x_in[zj].astype(F32)
        z_out[zj] = both.astype(BF16)
        z_send(step).start()

    x_out(zi).wait_recv()
    moe[...] += y_part[sp].astype(F32) + x_in[zi].astype(F32)

    @pl.loop(1, outer)
    def _(step):
        zj = lax.rem(zi + step, outer)
        remote(z_out.at[zj], z_in.at[zj], zs_send.at[0], zs_recv.at[zj], (sp, tp)).wait_recv()
        moe[...] += z_in[zj].astype(F32)

    result[...] = layer_norm(moe[...], n2g[...], n2b[...]).astype(BF16)

    for kind in range(PIECES):
        for step in range(1, pairs):
            weight_out(kind, step).wait_send()
            weight_mate(kind, pair_slot(step), step).wait_send()
        weight_mate(kind, tp, 0).wait_send()
    for step in range(1, tp_n):
        part_out(step).wait_send()

    @pl.loop(1, sp_n)
    def _(step):
        w_out(step).wait_send()

        @pl.when(sp + step < sp_n)
        def _():
            carry_out(step).wait_send()

    @pl.when(sp + 1 < sp_n)
    def _():
        halo_copy.wait_send()

    @pl.loop(1, outer)
    def _(step):
        ag_out(step).wait_send()
        z_send(step).wait_send()

    @pl.loop(0, outer)
    def _(step):
        forward(step * inner + xi).wait_send()
        x_out(step).wait_send()


def shards(
    dims,
    stream,
    recurrence_input,
    output_gate_input,
    convolution_taps,
    first_group_gates,
    second_group_gates,
    channel_decay,
    position_log_extra,
    recurrence_output_weight,
    first_norm_gain,
    first_norm_bias,
    routed_expert_index,
    routed_expert_weight,
    routed_gate_weight,
    routed_up_weight,
    routed_down_weight,
    shared_gate_weight,
    shared_up_weight,
    shared_down_weight,
    second_norm_gain,
    second_norm_bias,
):
    sp_n, tp_n, inner = dims
    outer = sp_n // inner
    length = recurrence_input.shape[0]
    chans = 2 * recurrence_input.shape[2]
    quarter, width = stream.shape
    fe = routed_gate_weight.shape[2]
    fs = shared_gate_weight.shape[1]
    vec = lambda a: a.reshape(1, width)
    vmem = pl.BlockSpec(memory_space=pltpu.VMEM)
    hbm = pl.BlockSpec(memory_space=pltpu.HBM)
    dma = pltpu.SemaphoreType.DMA
    block = (quarter, width)
    pairs = tp_n // 2
    operands = (
        stream,
        recurrence_input,
        output_gate_input,
        convolution_taps,
        first_group_gates,
        second_group_gates,
        channel_decay,
        position_log_extra,
        vec(first_norm_gain),
        vec(first_norm_bias),
        vec(second_norm_gain),
        vec(second_norm_bias),
        routed_expert_index.T,
        routed_expert_weight.T,
    )
    weights = (
        recurrence_output_weight.reshape(chans, width),
        routed_gate_weight.reshape(width, fe),
        routed_up_weight.reshape(width, fe),
        routed_down_weight.reshape(fe, width),
        shared_gate_weight,
        shared_up_weight,
        shared_down_weight,
    )
    limit = (28 + sp_n // 2) * 2**20
    operands = tuple(pltpu.with_memory_space_constraint(a, pltpu.HBM) for a in operands)
    weights = tuple(pltpu.with_memory_space_constraint(a, pltpu.HBM) for a in weights)
    return pl.pallas_call(
        functools.partial(kernel, dims),
        out_shape=jax.ShapeDtypeStruct(block, BF16),
        in_specs=[hbm] * (len(operands) + len(weights)),
        out_specs=vmem,
        scratch_shapes=[
            *(pltpu.VMEM(a.shape, a.dtype) for a in operands),
            dma((len(operands),)),
            pltpu.VMEM((length + 8, chans), F32),
            pltpu.VMEM((8,) + recurrence_input.shape[1:], BF16),
            pltpu.VMEM((2, chans), F32),
            pltpu.VMEM((sp_n, 2, chans), F32),
            pltpu.VMEM((sp_n, length), F32),
            pltpu.VMEM((sp_n, sp_n, length), F32),
            pltpu.VMEM((chans, width), BF16),
            pltpu.VMEM((tp_n, width, 2 * fe), BF16),
            pltpu.VMEM((tp_n, fe, width), BF16),
            pltpu.VMEM((width, 2 * fs), BF16),
            pltpu.VMEM((fs, width), BF16),
            pltpu.VMEM((tp_n,) + block, BF16),
            pltpu.VMEM((tp_n,) + block, BF16),
            pltpu.VMEM((sp_n,) + block, BF16),
            pltpu.VMEM((sp_n, quarter, tp_n * fe), BF16),
            pltpu.VMEM((sp_n,) + block, BF16),
            pltpu.VMEM((outer,) + block, BF16),
            pltpu.VMEM((outer,) + block, BF16),
            pltpu.VMEM((outer,) + block, BF16),
            pltpu.VMEM(block, F32),
            dma((8,)),
            dma((2,)),
            dma((sp_n,)),
            dma((sp_n,)),
            dma((sp_n,)),
            dma((sp_n,)),
            dma((PIECES, 2 * pairs)),
            dma((PIECES, tp_n)),
            dma((tp_n,)),
            dma((tp_n,)),
            dma((outer,)),
            dma((sp_n,)),
            dma((sp_n,)),
            dma((1,)),
            dma((outer,)),
            dma((outer,)),
            dma((outer,)),
            dma((outer,)),
        ],
        compiler_params=pltpu.CompilerParams(
            has_side_effects=True, collective_id=0, vmem_limit_bytes=limit
        ),
    )(*operands, *weights)


def solution(mesh):
    in_specs = (
        P(("sp", "tp"), None),
        P("sp", None, "tp"),
        P("sp", None, "tp"),
        P(None, None, "tp"),
        P(None, "tp", None, None),
        P(None, "tp", None, None),
        P(None, "tp"),
        P("sp", None, "tp"),
        P(None, "tp", None),
        P(),
        P(),
        P("sp", None),
        P("sp", None),
        P("sp", None, "tp"),
        P("sp", None, "tp"),
        P("sp", "tp", None),
        P(),
        P(),
        P(),
        P(),
        P(),
    )
    dims = (mesh.shape["sp"], mesh.shape["tp"], 2)
    return jax.shard_map(
        functools.partial(shards, dims),
        mesh=mesh,
        in_specs=in_specs,
        out_specs=P(("sp", "tp"), None),
        check_vma=False,
    )
```

```python
import functools

import jax
import jax.numpy as jnp
from jax import lax
from jax.experimental import pallas as pl
from jax.experimental.pallas import tpu as pltpu
from jax.sharding import PartitionSpec as P

RESIDUAL_SCALE = 8.0**0.25
NORM_EPSILON = 1e-05
LANES = 128
ROW_CUTS = 4
COLUMN_CUTS = 4
EARLY = 4
SPLITS = 2
MESH = pl.DeviceIdType.MESH
F32 = jnp.float32
BF16 = jnp.bfloat16


def layer_norm(values, gain, bias):
    row_mean = jnp.mean(values, axis=-1, keepdims=True)
    spread = jnp.mean(jnp.square(values - row_mean), axis=-1, keepdims=True)
    return (values - row_mean) * lax.rsqrt(spread + NORM_EPSILON) * gain + bias


def expm1_negative(z):
    small = jnp.full_like(z, 1.0 / 40320.0)
    for n in (5040.0, 720.0, 120.0, 24.0, 6.0, 2.0, 1.0):
        small = small * z + 1.0 / n
    return jnp.where(z > -0.5, small * z, jnp.exp(z) - 1.0)


def softplus(y):
    u = jnp.exp(-jnp.abs(y))
    s = u / (2.0 + u)
    sq = s * s
    series = jnp.full_like(s, 1.0 / 17.0)
    for n in (15.0, 13.0, 11.0, 9.0, 7.0, 5.0, 3.0, 1.0):
        series = series * sq + 1.0 / n
    return jnp.maximum(y, 0.0) + 2.0 * s * series


def lane_blocks(maps_ref):
    kinds, heads, size, _ = maps_ref.shape
    per = LANES // size
    blocks = []
    for start in range(0, heads, per):
        sides = []
        for kind in range(kinds):
            if per == 1:
                sides.append(maps_ref[kind, start])
                continue
            tall = []
            for p in range(per):
                row = lax.broadcasted_iota(jnp.int32, (size, LANES), 0)
                col = lax.broadcasted_iota(jnp.int32, (size, LANES), 1)
                place = jnp.where(col == row + p * size, 1.0, 0.0).astype(BF16)
                tall.append(dot(maps_ref[kind, start + p], place))
            sides.append(jnp.concatenate(tall, axis=0).astype(BF16))
        blocks.append(jnp.concatenate(sides, axis=1))
    return blocks


def silu(v):
    return v * jax.nn.sigmoid(v)


def dot(a, b):
    return jnp.dot(a, b, preferred_element_type=F32)


def kernel(
    dims,
    stream_hbm, rec_hbm, gate_hbm, taps_hbm, small_hbm, large_hbm, decay_hbm, extra_hbm,
    n1g_hbm, n1b_hbm, n2g_hbm, n2b_hbm, ids_hbm, wts_hbm,
    out_w_hbm, rg_hbm, ru_hbm, rd_hbm, sg_hbm, su_hbm, sd_hbm,
    result,
    stream, rec_in, gate_in, taps, small_maps, large_maps, channel_decay, extra, n1g, n1b, n2g, n2b,
    ids, wts, in_sem,
    padded, halo, carry_own, carry_in, wdense, w_in, w_rows, out_w, w_gu, w_d, s_gu, s_d,
    part, pair_in, pair_out, part_in, rows, hid, y_own, y_out, x_in, z_out, z_in, moe,
    local_sem, halo_sem, carry_send, carry_recv, w_send, w_recv,
    wt_send, wt_recv, pair_send, pair_recv, tp_send, tp_recv, right_send, left_send, fw_send, ag_recv,
    xs_send, xs_recv, zs_send, zs_recv,
):
    sp_n, tp_n, inner = dims
    outer = sp_n // inner
    pairs = tp_n // 2
    sp, tp = lax.axis_index("sp"), lax.axis_index("tp")
    zi, xi = sp // inner, lax.rem(sp, inner)
    other_x = lax.rem(xi + 1, inner)
    x_peer = zi * inner + other_x
    half_c = lax.rem(tp, 2)
    yi = tp // 2
    mate = yi * 2 + (1 - half_c)
    length = rec_in.shape[0]
    chans = rec_in.shape[1] * rec_in.shape[2]
    quarter, width = stream.shape
    fe = rg_hbm.shape[1]
    fs = sg_hbm.shape[1]
    cut = width // COLUMN_CUTS
    half_w = width // SPLITS

    def remote(src, dst, send, recv, where):
        return pltpu.make_async_remote_copy(
            src_ref=src, dst_ref=dst, send_sem=send, recv_sem=recv,
            device_id=where, device_id_type=MESH,
        )

    loads = [
        pltpu.make_async_copy(src, dst, in_sem.at[i])
        for i, (src, dst) in enumerate([
            (rec_hbm, rec_in), (small_hbm, small_maps), (large_hbm, large_maps), (taps_hbm, taps),
            (decay_hbm, channel_decay), (extra_hbm, extra), (gate_hbm, gate_in), (ids_hbm, ids),
            (wts_hbm, wts), (stream_hbm, stream), (n1g_hbm, n1g), (n1b_hbm, n1b), (n2g_hbm, n2g),
            (n2b_hbm, n2b),
        ])
    ]
    for load in loads:
        load.start()
    barrier = pltpu.get_barrier_semaphore()

    @pl.loop(1, sp_n)
    def _(step):
        pl.semaphore_signal(
            barrier, inc=1, device_id=(lax.rem(sp + step, sp_n), tp), device_id_type=MESH
        )

    for step in range(1, tp_n):
        pl.semaphore_signal(
            barrier, inc=1, device_id=(sp, lax.rem(tp + step, tp_n)), device_id_type=MESH
        )

    depth = rg_hbm.shape[0] // ROW_CUTS
    pieces = [(kind, part_id) for part_id in range(ROW_CUTS) for kind in (0, 1)]
    gate_pieces = len(pieces)
    pieces += [(2, part_id) for part_id in range(COLUMN_CUTS)]

    def weight_src(piece):
        kind, part_id = pieces[piece]
        if kind == 2:
            return rd_hbm.at[:, pl.ds(part_id * cut, cut)]
        return (rg_hbm, ru_hbm)[kind].at[pl.ds(part_id * depth, depth)]

    def weight_dst(slot, piece):
        kind, part_id = pieces[piece]
        if kind == 2:
            return w_d.at[part_id, slot]
        return w_gu.at[slot, pl.ds(part_id * depth, depth), pl.ds(kind * fe, fe)]

    def weight_out(piece, step):
        return remote(
            weight_src(piece), weight_dst(tp, piece),
            wt_send.at[piece, step], wt_recv.at[piece, tp],
            (sp, lax.rem(yi + step, pairs) * 2 + half_c),
        )

    def weight_mate(piece, slot, step):
        src = weight_src(piece) if step == 0 else weight_dst(slot, piece)
        return remote(
            src, weight_dst(slot, piece),
            wt_send.at[piece, pairs + step], wt_recv.at[piece, slot], (sp, mate),
        )

    def pair_slot(step):
        return lax.rem(yi + step, pairs) * 2 + half_c

    def weight_arrival(piece, slot):
        return remote(
            weight_dst(slot, piece), weight_dst(slot, piece),
            wt_send.at[piece, 0], wt_recv.at[piece, slot], (sp, mate),
        )

    def relay(piece):
        for step in range(1, pairs):
            weight_arrival(piece, pair_slot(step)).wait_recv()
            weight_mate(piece, pair_slot(step), step).start()

    def from_mate(piece):
        for step in range(pairs):
            weight_arrival(piece, lax.rem(yi + step, pairs) * 2 + 1 - half_c).wait_recv()

    locals_ = [pltpu.make_async_copy(out_w_hbm, out_w, local_sem.at[0])]
    locals_ += [
        pltpu.make_async_copy(weight_src(piece), weight_dst(tp, piece), local_sem.at[4 + piece])
        for piece in range(len(pieces))
    ]
    shared_loads = [
        pltpu.make_async_copy(sg_hbm, s_gu.at[:, pl.ds(0, fs)], local_sem.at[1]),
        pltpu.make_async_copy(su_hbm, s_gu.at[:, pl.ds(fs, fs)], local_sem.at[2]),
        pltpu.make_async_copy(sd_hbm, s_d, local_sem.at[3]),
    ]
    for load in locals_:
        load.start()
    for load in shared_loads:
        load.start()
    for load in loads:
        load.wait()
    pl.semaphore_wait(barrier, sp_n - 1 + tp_n - 1)

    halo_copy = remote(
        rec_in.at[pl.ds(length - 8, 8)], halo, halo_sem.at[0], halo_sem.at[1],
        (lax.rem(sp + 1, sp_n), tp),
    )

    @pl.when(sp + 1 < sp_n)
    def _():
        halo_copy.start()

    for piece in range(EARLY):
        for step in range(1, pairs):
            weight_out(piece, step).start()
    for piece in range(len(pieces)):
        weight_mate(piece, tp, 0).start()

    expert = lax.broadcasted_iota(jnp.int32, (wdense.shape[0], length), 0)
    table = jnp.zeros((wdense.shape[0], length), F32)
    for k in range(ids.shape[0]):
        table = table + jnp.where(expert == ids[k : k + 1], wts[k : k + 1], 0.0)
    wdense[...] = table
    w_in[sp] = table

    def w_out(step):
        return remote(
            wdense, w_in.at[sp], w_send.at[step], w_recv.at[sp], (lax.rem(sp + step, sp_n), tp)
        )

    small_blocks, large_blocks = lane_blocks(small_maps), lane_blocks(large_maps)
    rate_rows = -8.0 * softplus(-channel_decay[...])
    rate = jnp.concatenate([rate_rows[0:1], rate_rows[1:2]], axis=1)
    tap_rows = [
        jnp.concatenate([taps[k, 0:1], taps[k, 1:2]], axis=1).astype(F32)
        for k in range(taps.shape[0])
    ]

    padded[pl.ds(8, length)] = rec_in[...].astype(F32).reshape(length, chans)

    @pl.when(sp == 0)
    def _():
        padded[pl.ds(0, 8)] = jnp.zeros((8, chans), F32)

    @pl.when(sp > 0)
    def _():
        halo_copy.wait_recv()
        padded[pl.ds(0, 8)] = halo[...].astype(F32).reshape(8, chans)

    tap_n = taps.shape[0]
    summed = tap_rows[0] * padded[pl.ds(8 - tap_n + 1, length)]
    for k in range(1, tap_n):
        summed = summed + tap_rows[k] * padded[pl.ds(8 - tap_n + 1 + k, length)]
    conv = summed.astype(BF16)
    outs = [
        dot(conv[:, i * LANES : (i + 1) * LANES], maps)
        for i, maps in enumerate(small_blocks + large_blocks)
    ]
    recur = jax.nn.sigmoid(jnp.concatenate([o[:, :LANES] for o in outs], axis=1))
    inp = jax.nn.sigmoid(jnp.concatenate([o[:, LANES:] for o in outs], axis=1))
    log_decay = recur * rate + extra[...].reshape(length, chans)
    decay = jnp.exp(log_decay)
    state = jnp.sqrt(-expm1_negative(2.0 * log_decay)) * inp * conv.astype(F32)
    row_id = lax.broadcasted_iota(jnp.int32, (length, chans), 0)
    shift = 1
    while shift < length:
        live = row_id >= shift
        before_a = jnp.where(live, pltpu.roll(decay, shift, 0), 1.0)
        before_b = jnp.where(live, pltpu.roll(state, shift, 0), 0.0)
        state = decay * before_b + state
        decay = decay * before_a
        shift *= 2
    carry_own[...] = jnp.concatenate(
        [decay[length - 1 :], state[length - 1 :]], axis=0
    )

    def carry_out(step):
        return remote(
            carry_own, carry_in.at[sp], carry_send.at[step], carry_recv.at[sp],
            (lax.rem(sp + step, sp_n), tp),
        )

    def carry_arrival(who):
        return remote(
            carry_own, carry_in.at[who], carry_send.at[0], carry_recv.at[who], (sp, tp)
        )

    @pl.loop(1, sp_n)
    def _(back):
        step = sp_n - back

        @pl.when(sp + step < sp_n)
        def _():
            carry_out(step).start()

    @pl.loop(1, sp_n)
    def _(step):
        w_out(step).start()

    gi = gate_in[...].astype(F32).reshape(length, chans)
    gelu = 0.5 * gi * (1.0 + jnp.tanh(0.7978845608028654 * (gi + 0.044715 * gi * gi * gi)))

    def fold(who, incoming):
        carry_arrival(who).wait_recv()
        link = carry_in[who]
        return link[0:1] * incoming + link[1:2]

    incoming = lax.fori_loop(0, sp, fold, jnp.zeros((1, chans), F32))
    branch = (gelu * (state + decay * incoming)).astype(BF16)
    locals_[0].wait()
    part[...] = dot(branch, out_w[...]).astype(BF16).reshape(part.shape)

    def pair_copy(step):
        slot = lax.rem(yi + step, pairs) * 2 + 1 - half_c
        return remote(
            part.at[slot], pair_in.at[step], pair_send.at[step], pair_recv.at[step], (sp, mate)
        )

    def part_out(step):
        to = lax.rem(yi + step, pairs)
        return remote(
            pair_out.at[step], part_in.at[yi], tp_send.at[step], tp_recv.at[yi],
            (sp, to * 2 + half_c),
        )

    def part_arrival(who):
        return remote(
            pair_out.at[0], part_in.at[who], tp_send.at[0], tp_recv.at[who], (sp, mate)
        )

    for step in range(1, pairs + 1):
        pair_copy(step % pairs).start()
    for step in range(1, pairs):
        pair_copy(step).wait_recv()
        pair_out[step] = (
            part[pair_slot(step)].astype(F32) + pair_in[step].astype(F32)
        ).astype(BF16)
        part_out(step).start()
    for piece in range(EARLY, len(pieces)):
        for step in range(1, pairs):
            weight_out(piece, step).start()
    for piece in range(EARLY):
        relay(piece)
    pair_copy(0).wait_recv()
    mixed = part[tp].astype(F32) + pair_in[0].astype(F32)
    for step in range(1, pairs):
        who = lax.rem(yi + step, pairs)
        part_arrival(who).wait_recv()
        mixed = mixed + part_in[who].astype(F32)
    normed = layer_norm(
        RESIDUAL_SCALE * stream[...].astype(F32) + mixed, n1g[...], n1b[...]
    ).astype(BF16)
    rows[xi, zi] = normed

    def row_piece(col, zj, h):
        return rows.at[col, zj, :, pl.ds(h * half_w, half_w)]

    def row_copy(zj, h, sems, where):
        piece = row_piece(xi, zj, h)
        return remote(piece, piece, sems.at[zj, h], ag_recv.at[zj * inner + xi, h], (where, tp))

    def row_right(zj, h):
        return row_copy(zj, h, right_send, (zi + 1) * inner + xi)

    def row_left(zj, h):
        return row_copy(zj, h, left_send, (zi - 1) * inner + xi)

    def row_across(zj, h):
        return row_copy(zj, h, fw_send, x_peer)

    def row_arrival(col, zj, h):
        piece = row_piece(col, zj, h)
        return remote(
            piece, piece, fw_send.at[zj, h], ag_recv.at[zj * inner + col, h], (x_peer, tp)
        )

    for h in range(SPLITS):
        @pl.when(zi + 1 < outer)
        def _():
            row_right(zi, h).start()

        @pl.when(zi > 0)
        def _():
            row_left(zi, h).start()

        row_across(zi, h).start()

    @pl.loop(1, outer)
    def _(step):
        for h in range(SPLITS):
            @pl.when(zi - step >= 0)
            def _():
                row_arrival(xi, zi - step, h).wait_recv()

                @pl.when(zi + 1 < outer)
                def _():
                    row_right(zi - step, h).start()

                row_across(zi - step, h).start()

            @pl.when(zi + step < outer)
            def _():
                row_arrival(xi, zi + step, h).wait_recv()

                @pl.when(zi > 0)
                def _():
                    row_left(zi + step, h).start()

                row_across(zi + step, h).start()

    for piece in range(EARLY, gate_pieces):
        relay(piece)
    for load in shared_loads:
        load.wait()
    up = dot(normed, s_gu[...])
    s_hid = (silu(up[:, :fs]) * up[:, fs:]).astype(BF16)
    moe[...] = dot(s_hid, s_d[...]) + RESIDUAL_SCALE * normed.astype(F32)

    @pl.loop(1, sp_n)
    def _(step):
        who = lax.rem(sp + step, sp_n)
        remote(wdense, w_in.at[who], w_send.at[0], w_recv.at[who], (sp, tp)).wait_recv()

    own_rows = lax.broadcasted_iota(jnp.int32, (quarter, length), 0) + tp * quarter
    pick = lax.broadcasted_iota(jnp.int32, (quarter, length), 1) == own_rows

    @pl.loop(0, outer)
    def _(zj):
        for j in range(inner):
            line = w_in[zj * inner + j, pl.ds(sp, 1)]
            weight = jnp.sum(jnp.where(pick, line, 0.0), axis=1, keepdims=True)
            w_rows[j, zj] = jnp.broadcast_to(weight, (quarter, LANES))

    for load in locals_[1 : 1 + gate_pieces]:
        load.wait()
    for piece in range(gate_pieces):
        from_mate(piece)

    batch = min(outer, 4)

    def gate_up(col, i):
        block = rows[col, pl.ds(i * batch, batch)].reshape(batch * quarter, width)
        for t in range(tp_n):
            gu = dot(block, w_gu[t])
            act = (silu(gu[:, :fe]) * gu[:, fe:]).astype(BF16)
            hid[col, pl.ds(i * batch, batch), :, t * fe : (t + 1) * fe] = act.reshape(
                batch, quarter, fe
            )

    @pl.loop(0, outer // batch)
    def _(i):
        gate_up(xi, i)

    @pl.loop(0, outer)
    def _(zj):
        for h in range(SPLITS):
            row_arrival(other_x, zj, h).wait_recv()

    @pl.loop(0, outer // batch)
    def _(i):
        gate_up(other_x, i)

    def x_out(c, zj):
        return remote(
            y_out.at[c, zj], x_in.at[c, zj], xs_send.at[c, zj], xs_recv.at[c, zj], (x_peer, tp)
        )

    def z_send(c, step):
        zj = lax.rem(zi + step, outer)
        return remote(
            z_out.at[c, zj], z_in.at[c, zi], zs_send.at[c, step], zs_recv.at[c, zi],
            (zj * inner + xi, tp),
        )

    def down(c, col, dest):
        @pl.loop(0, outer // batch)
        def _(i):
            block = hid[col, pl.ds(i * batch, batch)].reshape(batch * quarter, tp_n * fe)
            value = dot(block, w_d[c].reshape(tp_n * fe, cut))
            weight = w_rows[col, pl.ds(i * batch, batch)].reshape(batch * quarter, LANES)
            for a in range(0, cut, LANES):
                dest[c, pl.ds(i * batch, batch), :, a : a + LANES] = (
                    (weight * value[:, a : a + LANES])
                    .astype(dest.dtype)
                    .reshape(batch, quarter, LANES)
                )

    def merge(c):
        @pl.loop(1, outer)
        def _(step):
            zj = lax.rem(zi + step, outer)
            x_out(c, zj).wait_recv()
            z_out[c, zj] = (y_own[c, zj].astype(F32) + x_in[c, zj].astype(F32)).astype(BF16)
            z_send(c, step).start()

    def settle(c):
        x_out(c, zi).wait_recv()
        here = moe[:, c * cut : (c + 1) * cut] + (
            y_own[c, zi].astype(F32) + x_in[c, zi].astype(F32)
        )
        moe[:, c * cut : (c + 1) * cut] = here

    for c in range(COLUMN_CUTS):
        piece = gate_pieces + c
        relay(piece)
        locals_[1 + piece].wait()
        from_mate(piece)
        down(c, other_x, y_out)

        @pl.loop(1, outer + 1)
        def _(step):
            x_out(c, lax.rem(zi + step, outer)).start()

        down(c, xi, y_own)
        if c:
            merge(c - 1)
            settle(c - 1)
    merge(COLUMN_CUTS - 1)
    settle(COLUMN_CUTS - 1)

    for c in range(COLUMN_CUTS):
        @pl.loop(1, outer)
        def _(step):
            zj = lax.rem(zi + step, outer)
            remote(
                z_out.at[c, zj], z_in.at[c, zj], zs_send.at[c, 0], zs_recv.at[c, zj], (sp, tp)
            ).wait_recv()
            moe[:, c * cut : (c + 1) * cut] += z_in[c, zj].astype(F32)

    result[...] = layer_norm(moe[...], n2g[...], n2b[...]).astype(BF16)

    for piece in range(len(pieces)):
        for step in range(1, pairs):
            weight_out(piece, step).wait_send()
            weight_mate(piece, pair_slot(step), step).wait_send()
        weight_mate(piece, tp, 0).wait_send()
    for step in range(pairs):
        pair_copy(step).wait_send()
    for step in range(1, pairs):
        part_out(step).wait_send()

    @pl.loop(1, sp_n)
    def _(step):
        w_out(step).wait_send()

        @pl.when(sp + step < sp_n)
        def _():
            carry_out(step).wait_send()

    @pl.when(sp + 1 < sp_n)
    def _():
        halo_copy.wait_send()

    @pl.loop(0, outer)
    def _(zj):
        for h in range(SPLITS):
            @pl.when(jnp.logical_and(zj <= zi, zi + 1 < outer))
            def _():
                row_right(zj, h).wait_send()

            @pl.when(jnp.logical_and(zj >= zi, zi > 0))
            def _():
                row_left(zj, h).wait_send()

            row_across(zj, h).wait_send()
        for c in range(COLUMN_CUTS):
            x_out(c, zj).wait_send()

    @pl.loop(1, outer)
    def _(step):
        for c in range(COLUMN_CUTS):
            z_send(c, step).wait_send()


def shards(
    dims,
    stream,
    recurrence_input,
    output_gate_input,
    convolution_taps,
    first_group_gates,
    second_group_gates,
    channel_decay,
    position_log_extra,
    recurrence_output_weight,
    first_norm_gain,
    first_norm_bias,
    routed_expert_index,
    routed_expert_weight,
    routed_gate_weight,
    routed_up_weight,
    routed_down_weight,
    shared_gate_weight,
    shared_up_weight,
    shared_down_weight,
    second_norm_gain,
    second_norm_bias,
):
    sp_n, tp_n, inner = dims
    outer = sp_n // inner
    length = recurrence_input.shape[0]
    chans = 2 * recurrence_input.shape[2]
    quarter, width = stream.shape
    fe = routed_gate_weight.shape[2]
    fs = shared_gate_weight.shape[1]
    vec = lambda a: a.reshape(1, width)
    vmem = pl.BlockSpec(memory_space=pltpu.VMEM)
    hbm = pl.BlockSpec(memory_space=pltpu.HBM)
    dma = pltpu.SemaphoreType.DMA
    block = (quarter, width)
    pairs = tp_n // 2
    cut = width // COLUMN_CUTS
    pieces = 2 * ROW_CUTS + COLUMN_CUTS
    operands = (
        stream,
        recurrence_input,
        output_gate_input,
        convolution_taps,
        first_group_gates,
        second_group_gates,
        channel_decay,
        position_log_extra,
        vec(first_norm_gain),
        vec(first_norm_bias),
        vec(second_norm_gain),
        vec(second_norm_bias),
        routed_expert_index.T,
        routed_expert_weight.T,
    )
    weights = (
        recurrence_output_weight.reshape(chans, width),
        routed_gate_weight.reshape(width, fe),
        routed_up_weight.reshape(width, fe),
        routed_down_weight.reshape(fe, width),
        shared_gate_weight,
        shared_up_weight,
        shared_down_weight,
    )
    limit = (28 + sp_n // 2) * 2**20
    operands = tuple(pltpu.with_memory_space_constraint(a, pltpu.HBM) for a in operands)
    weights = tuple(pltpu.with_memory_space_constraint(a, pltpu.HBM) for a in weights)
    return pl.pallas_call(
        functools.partial(kernel, dims),
        out_shape=jax.ShapeDtypeStruct(block, BF16),
        in_specs=[hbm] * (len(operands) + len(weights)),
        out_specs=vmem,
        scratch_shapes=[
            *(pltpu.VMEM(a.shape, a.dtype) for a in operands),
            dma((len(operands),)),
            pltpu.VMEM((length + 8, chans), F32),
            pltpu.VMEM((8,) + recurrence_input.shape[1:], BF16),
            pltpu.VMEM((2, chans), F32),
            pltpu.VMEM((sp_n, 2, chans), F32),
            pltpu.VMEM((sp_n, length), F32),
            pltpu.VMEM((sp_n, sp_n, length), F32),
            pltpu.VMEM((inner, outer, quarter, LANES), F32),
            pltpu.VMEM((chans, width), BF16),
            pltpu.VMEM((tp_n, width, 2 * fe), BF16),
            pltpu.VMEM((COLUMN_CUTS, tp_n, fe, cut), BF16),
            pltpu.VMEM((width, 2 * fs), BF16),
            pltpu.VMEM((fs, width), BF16),
            pltpu.VMEM((tp_n,) + block, BF16),
            pltpu.VMEM((pairs,) + block, BF16),
            pltpu.VMEM((pairs,) + block, BF16),
            pltpu.VMEM((pairs,) + block, BF16),
            pltpu.VMEM((inner, outer) + block, BF16),
            pltpu.VMEM((inner, outer, quarter, tp_n * fe), BF16),
            *(pltpu.VMEM((COLUMN_CUTS, outer, quarter, cut), BF16) for _ in range(5)),
            pltpu.VMEM(block, F32),
            dma((4 + pieces,)),
            dma((2,)),
            dma((sp_n,)),
            dma((sp_n,)),
            dma((sp_n,)),
            dma((sp_n,)),
            dma((pieces, 2 * pairs)),
            dma((pieces, tp_n)),
            dma((pairs,)),
            dma((pairs,)),
            dma((pairs,)),
            dma((pairs,)),
            dma((outer, SPLITS)),
            dma((outer, SPLITS)),
            dma((outer, SPLITS)),
            dma((sp_n, SPLITS)),
            *(dma((COLUMN_CUTS, outer)) for _ in range(4)),
        ],
        compiler_params=pltpu.CompilerParams(
            has_side_effects=True, collective_id=0, vmem_limit_bytes=limit
        ),
    )(*operands, *weights)


def solution(mesh):
    in_specs = (
        P(("sp", "tp"), None),
        P("sp", None, "tp"),
        P("sp", None, "tp"),
        P(None, None, "tp"),
        P(None, "tp", None, None),
        P(None, "tp", None, None),
        P(None, "tp"),
        P("sp", None, "tp"),
        P(None, "tp", None),
        P(),
        P(),
        P("sp", None),
        P("sp", None),
        P("sp", None, "tp"),
        P("sp", None, "tp"),
        P("sp", "tp", None),
        P(),
        P(),
        P(),
        P(),
        P(),
    )
    dims = (mesh.shape["sp"], mesh.shape["tp"], 2)
    return jax.shard_map(
        functools.partial(shards, dims),
        mesh=mesh,
        in_specs=in_specs,
        out_specs=P(("sp", "tp"), None),
        check_vma=False,
    )
```

```python
import functools

import jax
import jax.numpy as jnp
from jax import lax
from jax.experimental import pallas as pl
from jax.experimental.pallas import tpu as pltpu
from jax.sharding import PartitionSpec as P

RESIDUAL_SCALE = 8.0**0.25
NORM_EPSILON = 1e-05
LANES = 128
ROW_CUTS = 4
COLUMN_CUTS = (2, 2, 2, 2, 2, 2, 2, 2)
EARLY = (3, 1)
SPLITS = 2
MESH = pl.DeviceIdType.MESH
F32 = jnp.float32
BF16 = jnp.bfloat16


def layer_norm(values, gain, bias):
    row_mean = jnp.mean(values, axis=-1, keepdims=True)
    spread = jnp.mean(jnp.square(values - row_mean), axis=-1, keepdims=True)
    return (values - row_mean) * lax.rsqrt(spread + NORM_EPSILON) * gain + bias


def expm1_negative(z):
    small = jnp.full_like(z, 1.0 / 40320.0)
    for n in (5040.0, 720.0, 120.0, 24.0, 6.0, 2.0, 1.0):
        small = small * z + 1.0 / n
    return jnp.where(z > -0.5, small * z, jnp.exp(z) - 1.0)


def softplus(y):
    u = jnp.exp(-jnp.abs(y))
    s = u / (2.0 + u)
    sq = s * s
    series = jnp.full_like(s, 1.0 / 17.0)
    for n in (15.0, 13.0, 11.0, 9.0, 7.0, 5.0, 3.0, 1.0):
        series = series * sq + 1.0 / n
    return jnp.maximum(y, 0.0) + 2.0 * s * series


def lane_blocks(maps_ref):
    kinds, heads, size, _ = maps_ref.shape
    per = LANES // size
    blocks = []
    for start in range(0, heads, per):
        sides = []
        for kind in range(kinds):
            if per == 1:
                sides.append(maps_ref[kind, start])
                continue
            tall = []
            for p in range(per):
                row = lax.broadcasted_iota(jnp.int32, (size, LANES), 0)
                col = lax.broadcasted_iota(jnp.int32, (size, LANES), 1)
                place = jnp.where(col == row + p * size, 1.0, 0.0).astype(BF16)
                tall.append(dot(maps_ref[kind, start + p], place))
            sides.append(jnp.concatenate(tall, axis=0).astype(BF16))
        blocks.append(jnp.concatenate(sides, axis=1))
    return blocks


def silu(v):
    return v * jax.nn.sigmoid(v)


def dot(a, b):
    return jnp.dot(a, b, preferred_element_type=F32)


def kernel(
    dims,
    stream_hbm, rec_hbm, gate_hbm, taps_hbm, small_hbm, large_hbm, decay_hbm, extra_hbm,
    n1g_hbm, n1b_hbm, n2g_hbm, n2b_hbm, ids_hbm, wts_hbm,
    out_w_hbm, rg_hbm, ru_hbm, rd_hbm, sg_hbm, su_hbm, sd_hbm,
    result,
    stream, rec_in, gate_in, taps, small_maps, large_maps, channel_decay, extra, n1g, n1b, n2g, n2b,
    ids, wts, in_sem,
    padded, halo, carry_own, carry_in, wdense, w_in, w_rows, out_w, w_gu, w_d, s_gu, s_d,
    part, pair_in, pair_out, part_in, rows, hid, gu_acc, y_own, y_out, x_in, z_out, z_in, moe,
    local_sem, halo_sem, carry_send, carry_recv, w_send, w_recv,
    out_send, own_send, relay_send, own_recv, far_recv, relay_recv, pair_send, pair_recv,
    tp_send, tp_recv, right_send, left_send, fw_send, ag_recv, agx_recv,
    xs_send, xs_recv, zs_send, zs_recv,
):
    sp_n, tp_n, inner = dims
    outer = sp_n // inner
    pairs = tp_n // 2
    sp, tp = lax.axis_index("sp"), lax.axis_index("tp")
    zi, xi = sp // inner, lax.rem(sp, inner)
    other_x = lax.rem(xi + 1, inner)
    x_peer = zi * inner + other_x
    half_c = lax.rem(tp, 2)
    yi = tp // 2
    mate = yi * 2 + (1 - half_c)
    length = rec_in.shape[0]
    chans = rec_in.shape[1] * rec_in.shape[2]
    quarter, width = stream.shape
    fe = rg_hbm.shape[1]
    fs = sg_hbm.shape[1]
    unit = width // sum(COLUMN_CUTS)
    spans = []
    for c in range(len(COLUMN_CUTS)):
        spans.append((sum(COLUMN_CUTS[:c]) * unit, COLUMN_CUTS[c] * unit))
    half_w = width // SPLITS

    def remote(src, dst, send, recv, where):
        return pltpu.make_async_remote_copy(
            src_ref=src, dst_ref=dst, send_sem=send, recv_sem=recv,
            device_id=where, device_id_type=MESH,
        )

    barrier = pltpu.get_barrier_semaphore()
    for step in range(1, tp_n):
        pl.semaphore_signal(
            barrier, inc=1, device_id=(sp, lax.rem(tp + step, tp_n)), device_id_type=MESH
        )

    @pl.loop(1, sp_n)
    def _(step):
        pl.semaphore_signal(
            barrier, inc=1, device_id=(lax.rem(sp + step, sp_n), tp), device_id_type=MESH
        )

    loads = [
        pltpu.make_async_copy(src, dst, in_sem.at[i])
        for i, (src, dst) in enumerate([
            (rec_hbm, rec_in), (small_hbm, small_maps), (large_hbm, large_maps), (taps_hbm, taps),
            (decay_hbm, channel_decay), (extra_hbm, extra), (gate_hbm, gate_in), (ids_hbm, ids),
            (wts_hbm, wts), (stream_hbm, stream), (n1g_hbm, n1g), (n1b_hbm, n1b), (n2g_hbm, n2g),
            (n2b_hbm, n2b),
        ])
    ]
    for load in loads:
        load.start()

    depth = rg_hbm.shape[0] // ROW_CUTS
    pieces = [(kind, part_id) for part_id in range(ROW_CUTS) for kind in (0, 1)]
    gate_pieces = len(pieces)
    pieces += [(2, part_id) for part_id in range(len(spans))]

    def weight_src(piece):
        kind, part_id = pieces[piece]
        if kind == 2:
            return rd_hbm.at[:, pl.ds(*spans[part_id])]
        return (rg_hbm, ru_hbm)[kind].at[pl.ds(part_id * depth, depth)]

    def weight_dst(slot, piece):
        kind, part_id = pieces[piece]
        if kind == 2:
            return w_d.at[slot, :, pl.ds(*spans[part_id])]
        return w_gu.at[slot, pl.ds(part_id * depth, depth), pl.ds(kind * fe, fe)]

    def stage_ref(slot, stage):
        if stage < ROW_CUTS:
            return w_gu.at[slot, pl.ds(stage * depth, depth)]
        return w_d.at[slot, :, pl.ds(*spans[stage - ROW_CUTS])]

    def weight_all(slot, down):
        return (w_d if down else w_gu).at[slot]

    def weight_out(piece, step):
        kind, part_id = pieces[piece]
        stage = ROW_CUTS + part_id if kind == 2 else part_id
        return remote(
            weight_src(piece), weight_dst(tp, piece),
            out_send.at[kind // 2, step - 1], far_recv.at[stage, step - 1],
            (sp, lax.rem(yi + step, pairs) * 2 + half_c),
        )

    def pair_slot(step):
        return lax.rem(yi + step, pairs) * 2 + half_c

    def far_arrival(stage, step):
        block = stage_ref(pair_slot(step), stage)
        return remote(
            block, block, out_send.at[0, 0], far_recv.at[stage, pairs - step - 1], (sp, mate)
        )

    def stage_mate(stage, step):
        block = stage_ref(pair_slot(step), stage)
        return remote(
            block, block, relay_send.at[int(stage >= ROW_CUTS), step - 1],
            relay_recv.at[stage, step - 1], (sp, mate),
        )

    def relay_arrival(stage, step):
        block = stage_ref(lax.rem(yi + step, pairs) * 2 + 1 - half_c, stage)
        return remote(
            block, block, relay_send.at[0, 0], relay_recv.at[stage, step - 1], (sp, mate)
        )

    def relay(stage):
        for step in range(1, pairs):
            far_arrival(stage, step).wait_recv()
            stage_mate(stage, step).start()

    def from_mate(stage):
        for step in range(1, pairs):
            relay_arrival(stage, step).wait_recv()

    own_weights = [
        (rg_hbm, w_gu.at[tp, :, pl.ds(0, fe)], 0),
        (ru_hbm, w_gu.at[tp, :, pl.ds(fe, fe)], 0),
        (rd_hbm, w_d.at[tp], 1),
    ]
    halo_copy = remote(
        rec_in.at[pl.ds(length - 8, 8)], halo, halo_sem.at[0], halo_sem.at[1],
        (lax.rem(sp + 1, sp_n), tp),
    )
    pl.semaphore_wait(barrier, sp_n - 1 + tp_n - 1)
    early = [*range(EARLY[0]), *range(gate_pieces, gate_pieces + EARLY[1])]
    for piece in early:
        for step in range(1, pairs):
            weight_out(piece, step).start()
    loads[0].wait()

    @pl.when(sp + 1 < sp_n)
    def _():
        halo_copy.start()

    out_w_load = pltpu.make_async_copy(out_w_hbm, out_w, local_sem.at[0])
    out_w_load.start()
    for src, dst, down in own_weights:
        remote(src, dst, own_send.at[down], own_recv.at[down], (sp, mate)).start()
        pltpu.make_async_copy(src, dst, local_sem.at[1 + down]).start()
    shared_loads = [
        pltpu.make_async_copy(sg_hbm, s_gu.at[:, pl.ds(0, fs)], local_sem.at[3]),
        pltpu.make_async_copy(su_hbm, s_gu.at[:, pl.ds(fs, fs)], local_sem.at[4]),
        pltpu.make_async_copy(sd_hbm, s_d, local_sem.at[5]),
    ]
    for load in shared_loads:
        load.start()
    for load in loads[1:]:
        load.wait()

    expert = lax.broadcasted_iota(jnp.int32, (wdense.shape[0], length), 0)
    table = jnp.zeros((wdense.shape[0], length), F32)
    for k in range(ids.shape[0]):
        table = table + jnp.where(expert == ids[k : k + 1], wts[k : k + 1], 0.0)
    wdense[...] = table
    w_in[sp] = table

    def w_out(step):
        return remote(
            wdense, w_in.at[sp], w_send.at[0], w_recv.at[0], (lax.rem(sp + step, sp_n), tp)
        )

    small_blocks, large_blocks = lane_blocks(small_maps), lane_blocks(large_maps)
    rate_rows = -8.0 * softplus(-channel_decay[...])
    rate = jnp.concatenate([rate_rows[0:1], rate_rows[1:2]], axis=1)
    tap_rows = [
        jnp.concatenate([taps[k, 0:1], taps[k, 1:2]], axis=1).astype(F32)
        for k in range(taps.shape[0])
    ]

    padded[pl.ds(8, length)] = rec_in[...].astype(F32).reshape(length, chans)

    @pl.when(sp == 0)
    def _():
        padded[pl.ds(0, 8)] = jnp.zeros((8, chans), F32)

    @pl.when(sp > 0)
    def _():
        halo_copy.wait_recv()
        padded[pl.ds(0, 8)] = halo[...].astype(F32).reshape(8, chans)

    tap_n = taps.shape[0]
    summed = tap_rows[0] * padded[pl.ds(8 - tap_n + 1, length)]
    for k in range(1, tap_n):
        summed = summed + tap_rows[k] * padded[pl.ds(8 - tap_n + 1 + k, length)]
    conv = summed.astype(BF16)
    outs = [
        dot(conv[:, i * LANES : (i + 1) * LANES], maps)
        for i, maps in enumerate(small_blocks + large_blocks)
    ]
    recur = jax.nn.sigmoid(jnp.concatenate([o[:, :LANES] for o in outs], axis=1))
    inp = jax.nn.sigmoid(jnp.concatenate([o[:, LANES:] for o in outs], axis=1))
    log_decay = recur * rate + extra[...].reshape(length, chans)
    decay = jnp.exp(log_decay)
    state = jnp.sqrt(-expm1_negative(2.0 * log_decay)) * inp * conv.astype(F32)
    row_id = lax.broadcasted_iota(jnp.int32, (length, chans), 0)
    shift = 1
    while shift < length:
        live = row_id >= shift
        before_a = jnp.where(live, pltpu.roll(decay, shift, 0), 1.0)
        before_b = jnp.where(live, pltpu.roll(state, shift, 0), 0.0)
        state = decay * before_b + state
        decay = decay * before_a
        shift *= 2
    carry_own[...] = jnp.concatenate(
        [decay[length - 1 :], state[length - 1 :]], axis=0
    )

    def carry_out(step):
        return remote(
            carry_own, carry_in.at[sp], carry_send.at[step], carry_recv.at[sp],
            (lax.rem(sp + step, sp_n), tp),
        )

    def carry_arrival(who):
        return remote(
            carry_own, carry_in.at[who], carry_send.at[0], carry_recv.at[who], (sp, tp)
        )

    @pl.loop(1, sp_n)
    def _(back):
        step = sp_n - back

        @pl.when(sp + step < sp_n)
        def _():
            carry_out(step).start()

    @pl.loop(1, sp_n)
    def _(step):
        w_out(step).start()

    gi = gate_in[...].astype(F32).reshape(length, chans)
    gelu = 0.5 * gi * (1.0 + jnp.tanh(0.7978845608028654 * (gi + 0.044715 * gi * gi * gi)))

    def fold(who, incoming):
        carry_arrival(who).wait_recv()
        link = carry_in[who]
        return link[0:1] * incoming + link[1:2]

    incoming = lax.fori_loop(0, sp, fold, jnp.zeros((1, chans), F32))
    branch = (gelu * (state + decay * incoming)).astype(BF16)
    out_w_load.wait()
    part[...] = dot(branch, out_w[...]).astype(BF16).reshape(part.shape)

    def pair_copy(step):
        slot = lax.rem(yi + step, pairs) * 2 + 1 - half_c
        return remote(
            part.at[slot], pair_in.at[step], pair_send.at[0], pair_recv.at[step], (sp, mate)
        )

    def part_out(step):
        to = lax.rem(yi + step, pairs)
        return remote(
            pair_out.at[step], part_in.at[yi], tp_send.at[step - 1], tp_recv.at[step - 1],
            (sp, to * 2 + half_c),
        )

    def part_arrival(step):
        who = lax.rem(yi + step, pairs)
        return remote(
            pair_out.at[0], part_in.at[who], tp_send.at[0], tp_recv.at[pairs - step - 1], (sp, mate)
        )

    for step in range(1, pairs + 1):
        pair_copy(step % pairs).start()
    for step in range(1, pairs):
        pair_copy(step).wait_recv()
        pair_out[step] = (
            part[pair_slot(step)].astype(F32) + pair_in[step].astype(F32)
        ).astype(BF16)
        part_out(step).start()
    for piece in range(len(pieces)):
        if piece not in early:
            for step in range(1, pairs):
                weight_out(piece, step).start()
    pair_copy(0).wait_recv()
    mixed = part[tp].astype(F32) + pair_in[0].astype(F32)
    for step in range(1, pairs):
        who = lax.rem(yi + step, pairs)
        part_arrival(step).wait_recv()
        mixed = mixed + part_in[who].astype(F32)
    normed = layer_norm(
        RESIDUAL_SCALE * stream[...].astype(F32) + mixed, n1g[...], n1b[...]
    ).astype(BF16)
    rows[xi, zi] = normed

    def row_piece(col, zj, h):
        return rows.at[col, zj, :, pl.ds(h * half_w, half_w)]

    def row_copy(zj, h, sems, where):
        piece = row_piece(xi, zj, h)
        return remote(piece, piece, sems, ag_recv.at[zj, h], (where, tp))

    def row_right(zj, h):
        return row_copy(zj, h, right_send.at[zj], (zi + 1) * inner + xi)

    def row_left(zj, h):
        return row_copy(zj, h, left_send.at[zj], (zi - 1) * inner + xi)

    def row_across(zj, h):
        piece = row_piece(xi, zj, h)
        return remote(piece, piece, fw_send.at[0], agx_recv.at[0], (x_peer, tp))

    def row_arrival(zj, h):
        piece = row_piece(xi, zj, h)
        return remote(piece, piece, fw_send.at[0], ag_recv.at[zj, h], (x_peer, tp))

    for h in range(SPLITS):
        @pl.when(zi + 1 < outer)
        def _():
            row_right(zi, h).start()

        @pl.when(zi > 0)
        def _():
            row_left(zi, h).start()

        row_across(zi, h).start()

    @pl.loop(1, outer)
    def _(step):
        for h in range(SPLITS):
            @pl.when(zi - step >= 0)
            def _():
                row_arrival(zi - step, h).wait_recv()

                @pl.when(zi + 1 < outer)
                def _():
                    row_right(zi - step, h).start()

                row_across(zi - step, h).start()

            @pl.when(zi + step < outer)
            def _():
                row_arrival(zi + step, h).wait_recv()

                @pl.when(zi > 0)
                def _():
                    row_left(zi + step, h).start()

                row_across(zi + step, h).start()

    for stage in (*range(ROW_CUTS - 1), *range(ROW_CUTS, ROW_CUTS + EARLY[1])):
        relay(stage)
    for load in shared_loads:
        load.wait()
    up = dot(normed, s_gu[...])
    s_hid = (silu(up[:, :fs]) * up[:, fs:]).astype(BF16)
    moe[...] = dot(s_hid, s_d[...]) + RESIDUAL_SCALE * normed.astype(F32)

    tables = w_in.at[pl.ds(0, sp_n - 1)]
    remote(tables, tables, w_send.at[0], w_recv.at[0], (x_peer, tp)).wait_recv()

    own_rows = lax.broadcasted_iota(jnp.int32, (quarter, length), 0) + tp * quarter
    pick = lax.broadcasted_iota(jnp.int32, (quarter, length), 1) == own_rows

    @pl.loop(0, outer)
    def _(zj):
        for j in range(inner):
            line = w_in[zj * inner + j, pl.ds(sp, 1)]
            weight = jnp.sum(jnp.where(pick, line, 0.0), axis=1, keepdims=True)
            w_rows[j, zj] = jnp.broadcast_to(weight, (quarter, LANES))

    for down in (0, 1):
        own = weight_all(tp, down)
        pltpu.make_async_copy(own, own, local_sem.at[1 + down]).wait()
        theirs = weight_all(mate, down)
        remote(theirs, theirs, own_send.at[down], own_recv.at[down], (sp, mate)).wait_recv()

    batch = min(outer, 4)
    tall = batch * quarter

    def gate_up(col, stage):
        last = stage == ROW_CUTS - 1

        @pl.loop(0, outer // batch)
        def _(i):
            block = rows[
                col, pl.ds(i * batch, batch), :, stage * depth : (stage + 1) * depth
            ].reshape(tall, depth)
            for t in range(tp_n):
                gu = dot(block, w_gu[t, stage * depth : (stage + 1) * depth])
                if stage:
                    gu = gu + gu_acc[col, i, :, t * 2 * fe : (t + 1) * 2 * fe]
                if last:
                    act = (silu(gu[:, :fe]) * gu[:, fe:]).astype(BF16)
                    hid[col, i, :, t * fe : (t + 1) * fe] = act
                else:
                    gu_acc[col, i, :, t * 2 * fe : (t + 1) * 2 * fe] = gu

    for stage in range(ROW_CUTS - 1):
        from_mate(stage)
        gate_up(xi, stage)
    side = rows.at[other_x]
    remote(side, side, fw_send.at[0], agx_recv.at[0], (x_peer, tp)).wait_recv()
    for stage in range(ROW_CUTS - 1):
        gate_up(other_x, stage)
    relay(ROW_CUTS - 1)
    from_mate(ROW_CUTS - 1)
    gate_up(other_x, ROW_CUTS - 1)
    gate_up(xi, ROW_CUTS - 1)

    def columns(ref, c):
        return ref.at[:, :, pl.ds(*spans[c])]

    def x_out(c):
        return remote(
            columns(y_out, c), columns(x_in, c), xs_send.at[0], xs_recv.at[c], (x_peer, tp)
        )

    def z_send(c, step):
        zj = lax.rem(zi + step, outer)
        return remote(
            columns(z_out, c).at[zj], columns(z_in, c).at[zi], zs_send.at[0], zs_recv.at[c],
            (zj * inner + xi, tp),
        )

    def down(c, col, dest):
        first, wide = spans[c]

        @pl.loop(0, outer // batch)
        def _(i):
            value = dot(
                hid[col, i], w_d[:, :, first : first + wide].reshape(tp_n * fe, wide)
            )
            weight = w_rows[col, pl.ds(i * batch, batch)].reshape(tall, LANES)
            for a in range(0, wide, LANES):
                dest[pl.ds(i * batch, batch), :, first + a : first + a + LANES] = (
                    (weight * value[:, a : a + LANES])
                    .astype(dest.dtype)
                    .reshape(batch, quarter, LANES)
                )

    def merge(c):
        first, wide = spans[c]
        at = slice(first, first + wide)
        x_out(c).wait_recv()

        @pl.loop(1, outer)
        def _(step):
            zj = lax.rem(zi + step, outer)
            z_out[zj, :, at] = (
                y_own[zj, :, at].astype(F32) + x_in[zj, :, at].astype(F32)
            ).astype(BF16)
            z_send(c, step).start()

        moe[:, at] = moe[:, at] + (y_own[zi, :, at].astype(F32) + x_in[zi, :, at].astype(F32))

    chunks = len(spans)
    ahead = max(EARLY[1], 1)
    if EARLY[1] == 0:
        relay(ROW_CUTS)
    for c in range(chunks):
        if ahead <= c + 1 < chunks:
            relay(ROW_CUTS + c + 1)
        from_mate(ROW_CUTS + c)
        down(c, other_x, y_out)
        x_out(c).start()
        down(c, xi, y_own)
        if c >= 2:
            merge(c - 2)
    merge(chunks - 2)
    merge(chunks - 1)

    for c in range(chunks):
        first, wide = spans[c]
        at = slice(first, first + wide)
        group = columns(z_in, c).at[pl.ds(0, outer - 1)]
        remote(group, group, zs_send.at[0], zs_recv.at[c], (x_peer, tp)).wait_recv()

        @pl.loop(1, outer)
        def _(step):
            moe[:, at] += z_in[lax.rem(zi + step, outer), :, at].astype(F32)

    result[...] = layer_norm(moe[...], n2g[...], n2b[...]).astype(BF16)

    for down in (0, 1):
        whole = weight_all(tp, down)
        for step in range(1, pairs):
            remote(whole, whole, out_send.at[down, step - 1], own_recv.at[0], (sp, mate)).wait_send()
            remote(
                whole, whole, relay_send.at[down, step - 1], own_recv.at[0], (sp, mate)
            ).wait_send()
        remote(whole, whole, own_send.at[down], own_recv.at[0], (sp, mate)).wait_send()
    remote(pair_in, pair_in, pair_send.at[0], pair_recv.at[0], (sp, mate)).wait_send()
    for step in range(1, pairs):
        part_out(step).wait_send()
    remote(tables, tables, w_send.at[0], w_recv.at[0], (x_peer, tp)).wait_send()

    @pl.loop(1, sp_n)
    def _(step):
        @pl.when(sp + step < sp_n)
        def _():
            carry_out(step).wait_send()

    @pl.when(sp + 1 < sp_n)
    def _():
        halo_copy.wait_send()

    @pl.loop(0, outer)
    def _(zj):
        block = rows.at[xi, zj]

        @pl.when(jnp.logical_and(zj <= zi, zi + 1 < outer))
        def _():
            remote(block, block, right_send.at[zj], fw_send.at[0], (x_peer, tp)).wait_send()

        @pl.when(jnp.logical_and(zj >= zi, zi > 0))
        def _():
            remote(block, block, left_send.at[zj], fw_send.at[0], (x_peer, tp)).wait_send()

    remote(side, side, fw_send.at[0], agx_recv.at[0], (x_peer, tp)).wait_send()
    remote(y_out, y_out, xs_send.at[0], agx_recv.at[0], (x_peer, tp)).wait_send()
    sent = z_out.at[pl.ds(0, outer - 1)]
    remote(sent, sent, zs_send.at[0], agx_recv.at[0], (x_peer, tp)).wait_send()


def shards(
    dims,
    stream,
    recurrence_input,
    output_gate_input,
    convolution_taps,
    first_group_gates,
    second_group_gates,
    channel_decay,
    position_log_extra,
    recurrence_output_weight,
    first_norm_gain,
    first_norm_bias,
    routed_expert_index,
    routed_expert_weight,
    routed_gate_weight,
    routed_up_weight,
    routed_down_weight,
    shared_gate_weight,
    shared_up_weight,
    shared_down_weight,
    second_norm_gain,
    second_norm_bias,
):
    sp_n, tp_n, inner = dims
    outer = sp_n // inner
    length = recurrence_input.shape[0]
    chans = 2 * recurrence_input.shape[2]
    quarter, width = stream.shape
    fe = routed_gate_weight.shape[2]
    fs = shared_gate_weight.shape[1]
    vec = lambda a: a.reshape(1, width)
    vmem = pl.BlockSpec(memory_space=pltpu.VMEM)
    hbm = pl.BlockSpec(memory_space=pltpu.HBM)
    dma = pltpu.SemaphoreType.DMA
    block = (quarter, width)
    pairs = tp_n // 2
    stages = ROW_CUTS + len(COLUMN_CUTS)
    batch = min(outer, 4)
    operands = (
        stream,
        recurrence_input,
        output_gate_input,
        convolution_taps,
        first_group_gates,
        second_group_gates,
        channel_decay,
        position_log_extra,
        vec(first_norm_gain),
        vec(first_norm_bias),
        vec(second_norm_gain),
        vec(second_norm_bias),
        routed_expert_index.T,
        routed_expert_weight.T,
    )
    weights = (
        recurrence_output_weight.reshape(chans, width),
        routed_gate_weight.reshape(width, fe),
        routed_up_weight.reshape(width, fe),
        routed_down_weight.reshape(fe, width),
        shared_gate_weight,
        shared_up_weight,
        shared_down_weight,
    )
    limit = (28 + sp_n // 2) * 2**20
    operands = tuple(pltpu.with_memory_space_constraint(a, pltpu.HBM) for a in operands)
    weights = tuple(pltpu.with_memory_space_constraint(a, pltpu.HBM) for a in weights)
    return pl.pallas_call(
        functools.partial(kernel, dims),
        out_shape=jax.ShapeDtypeStruct(block, BF16),
        in_specs=[hbm] * (len(operands) + len(weights)),
        out_specs=vmem,
        scratch_shapes=[
            *(pltpu.VMEM(a.shape, a.dtype) for a in operands),
            dma((len(operands),)),
            pltpu.VMEM((length + 8, chans), F32),
            pltpu.VMEM((8,) + recurrence_input.shape[1:], BF16),
            pltpu.VMEM((2, chans), F32),
            pltpu.VMEM((sp_n, 2, chans), F32),
            pltpu.VMEM((sp_n, length), F32),
            pltpu.VMEM((sp_n, sp_n, length), F32),
            pltpu.VMEM((inner, outer, quarter, LANES), F32),
            pltpu.VMEM((chans, width), BF16),
            pltpu.VMEM((tp_n, width, 2 * fe), BF16),
            pltpu.VMEM((tp_n, fe, width), BF16),
            pltpu.VMEM((width, 2 * fs), BF16),
            pltpu.VMEM((fs, width), BF16),
            pltpu.VMEM((tp_n,) + block, BF16),
            pltpu.VMEM((pairs,) + block, BF16),
            pltpu.VMEM((pairs,) + block, BF16),
            pltpu.VMEM((pairs,) + block, BF16),
            pltpu.VMEM((inner, outer) + block, BF16),
            pltpu.VMEM((inner, outer // batch, batch * quarter, tp_n * fe), BF16),
            pltpu.VMEM((inner, outer // batch, batch * quarter, tp_n * 2 * fe), F32),
            *(pltpu.VMEM((outer,) + block, BF16) for _ in range(5)),
            pltpu.VMEM(block, F32),
            dma((6,)),
            dma((2,)),
            dma((sp_n,)),
            dma((sp_n,)),
            dma((1,)),
            dma((1,)),
            dma((2, pairs - 1)),
            dma((2,)),
            dma((2, pairs - 1)),
            dma((2,)),
            dma((stages, pairs - 1)),
            dma((stages, pairs - 1)),
            dma((1,)),
            dma((pairs,)),
            dma((pairs - 1,)),
            dma((pairs - 1,)),
            dma((outer,)),
            dma((outer,)),
            dma((1,)),
            dma((outer, SPLITS)),
            dma((1,)),
            dma((1,)),
            dma((len(COLUMN_CUTS),)),
            dma((1,)),
            dma((len(COLUMN_CUTS),)),
        ],
        compiler_params=pltpu.CompilerParams(
            has_side_effects=True, collective_id=0, vmem_limit_bytes=limit
        ),
    )(*operands, *weights)


def solution(mesh):
    in_specs = (
        P(("sp", "tp"), None),
        P("sp", None, "tp"),
        P("sp", None, "tp"),
        P(None, None, "tp"),
        P(None, "tp", None, None),
        P(None, "tp", None, None),
        P(None, "tp"),
        P("sp", None, "tp"),
        P(None, "tp", None),
        P(),
        P(),
        P("sp", None),
        P("sp", None),
        P("sp", None, "tp"),
        P("sp", None, "tp"),
        P("sp", "tp", None),
        P(),
        P(),
        P(),
        P(),
        P(),
    )
    dims = (mesh.shape["sp"], mesh.shape["tp"], 2)
    return jax.shard_map(
        functools.partial(shards, dims),
        mesh=mesh,
        in_specs=in_specs,
        out_specs=P(("sp", "tp"), None),
        check_vma=False,
    )
```

```python
import functools

import jax
import jax.numpy as jnp
from jax import lax
from jax.experimental import pallas as pl
from jax.experimental.pallas import tpu as pltpu
from jax.sharding import PartitionSpec as P

RESIDUAL_SCALE = 8.0**0.25
NORM_EPSILON = 1e-05
LANES = 128
ROW_CUTS = 4
COLUMN_CUTS = (2, 2, 2, 2, 2, 2, 2, 2)
EARLY = (0, 1, 1, 1)
SPLITS = 2
MESH = pl.DeviceIdType.MESH
F32 = jnp.float32
BF16 = jnp.bfloat16


def layer_norm(values, gain, bias):
    row_mean = jnp.mean(values, axis=-1, keepdims=True)
    spread = jnp.mean(jnp.square(values - row_mean), axis=-1, keepdims=True)
    return (values - row_mean) * lax.rsqrt(spread + NORM_EPSILON) * gain + bias


def expm1_negative(z):
    small = jnp.full_like(z, 1.0 / 40320.0)
    for n in (5040.0, 720.0, 120.0, 24.0, 6.0, 2.0, 1.0):
        small = small * z + 1.0 / n
    return jnp.where(z > -0.5, small * z, jnp.exp(z) - 1.0)


def softplus(y):
    u = jnp.exp(-jnp.abs(y))
    s = u / (2.0 + u)
    sq = s * s
    series = jnp.full_like(s, 1.0 / 17.0)
    for n in (15.0, 13.0, 11.0, 9.0, 7.0, 5.0, 3.0, 1.0):
        series = series * sq + 1.0 / n
    return jnp.maximum(y, 0.0) + 2.0 * s * series


def lane_blocks(maps_ref):
    kinds, heads, size, _ = maps_ref.shape
    per = LANES // size
    blocks = []
    for start in range(0, heads, per):
        sides = []
        for kind in range(kinds):
            if per == 1:
                sides.append(maps_ref[kind, start])
                continue
            tall = []
            for p in range(per):
                row = lax.broadcasted_iota(jnp.int32, (size, LANES), 0)
                col = lax.broadcasted_iota(jnp.int32, (size, LANES), 1)
                place = jnp.where(col == row + p * size, 1.0, 0.0).astype(BF16)
                tall.append(dot(maps_ref[kind, start + p], place))
            sides.append(jnp.concatenate(tall, axis=0).astype(BF16))
        blocks.append(jnp.concatenate(sides, axis=1))
    return blocks


def silu(v):
    return v * jax.nn.sigmoid(v)


def dot(a, b):
    return jnp.dot(a, b, preferred_element_type=F32)


def kernel(
    dims,
    stream_hbm, rec_hbm, gate_hbm, taps_hbm, small_hbm, large_hbm, decay_hbm, extra_hbm,
    n1g_hbm, n1b_hbm, n2g_hbm, n2b_hbm, ids_hbm, wts_hbm,
    out_w_hbm, rg_hbm, ru_hbm, rd_hbm, sg_hbm, su_hbm, sd_hbm,
    result,
    stream, rec_in, gate_in, taps, small_maps, large_maps, channel_decay, extra, n1g, n1b, n2g, n2b,
    ids, wts, in_sem,
    padded, halo, carry_own, carry_in, wdense, w_in, w_rows, w_peer, place_out, place_in, out_w, w_gu, w_d, s_gu, s_d,
    part, pair_in, pair_out, part_in, rows, hid, hid_pack, gu_acc, y_own, y_out, x_in, z_out, z_in, moe,
    local_sem, halo_sem, carry_send, carry_recv, w_send, w_recv,
    out_send, own_send, relay_send, own_recv, far_recv, relay_recv, pair_send, pair_recv,
    tp_send, tp_recv, right_send, left_send, fw_send, ag_recv, agx_recv,
    xs_send, xs_recv, zs_send, zs_recv,
):
    sp_n, tp_n, inner = dims
    outer = sp_n // inner
    pairs = tp_n // 2
    sp, tp = lax.axis_index("sp"), lax.axis_index("tp")
    zi, xi = sp // inner, lax.rem(sp, inner)
    other_x = lax.rem(xi + 1, inner)
    x_peer = zi * inner + other_x
    half_c = lax.rem(tp, 2)
    yi = tp // 2
    mate = yi * 2 + (1 - half_c)
    length = rec_in.shape[0]
    chans = rec_in.shape[1] * rec_in.shape[2]
    quarter, width = stream.shape
    fe = rg_hbm.shape[1]
    fs = sg_hbm.shape[1]
    unit = width // sum(COLUMN_CUTS)
    spans = []
    for c in range(len(COLUMN_CUTS)):
        spans.append((sum(COLUMN_CUTS[:c]) * unit, COLUMN_CUTS[c] * unit))
    half_w = width // SPLITS

    def remote(src, dst, send, recv, where):
        return pltpu.make_async_remote_copy(
            src_ref=src, dst_ref=dst, send_sem=send, recv_sem=recv,
            device_id=where, device_id_type=MESH,
        )

    barrier = pltpu.get_barrier_semaphore()
    for step in range(1, tp_n):
        pl.semaphore_signal(
            barrier, inc=1, device_id=(sp, lax.rem(tp + step, tp_n)), device_id_type=MESH
        )

    @pl.loop(1, sp_n)
    def _(step):
        pl.semaphore_signal(
            barrier, inc=1, device_id=(lax.rem(sp + step, sp_n), tp), device_id_type=MESH
        )

    loads = [
        pltpu.make_async_copy(src, dst, in_sem.at[i])
        for i, (src, dst) in enumerate([
            (rec_hbm, rec_in), (small_hbm, small_maps), (large_hbm, large_maps), (taps_hbm, taps),
            (decay_hbm, channel_decay), (extra_hbm, extra), (gate_hbm, gate_in), (ids_hbm, ids),
            (wts_hbm, wts), (stream_hbm, stream), (n1g_hbm, n1g), (n1b_hbm, n1b), (n2g_hbm, n2g),
            (n2b_hbm, n2b),
        ])
    ]
    for load in loads:
        load.start()

    depth = rg_hbm.shape[0] // ROW_CUTS
    pieces = [(kind, part_id) for part_id in range(ROW_CUTS) for kind in (0, 1)]
    gate_pieces = len(pieces)
    pieces += [(2, part_id) for part_id in range(len(spans))]

    def weight_src(piece):
        kind, part_id = pieces[piece]
        if kind == 2:
            return rd_hbm.at[:, pl.ds(*spans[part_id])]
        return (rg_hbm, ru_hbm)[kind].at[pl.ds(part_id * depth, depth)]

    def weight_dst(slot, piece):
        kind, part_id = pieces[piece]
        if kind == 2:
            return w_d.at[slot, :, pl.ds(*spans[part_id])]
        return w_gu.at[slot, pl.ds(part_id * depth, depth), pl.ds(kind * fe, fe)]

    def stage_ref(slot, stage):
        if stage < ROW_CUTS:
            return w_gu.at[slot, pl.ds(stage * depth, depth)]
        return w_d.at[slot, :, pl.ds(*spans[stage - ROW_CUTS])]

    def weight_all(slot, down):
        return (w_d if down else w_gu).at[slot]

    def weight_out(piece, step):
        kind, part_id = pieces[piece]
        stage = ROW_CUTS + part_id if kind == 2 else part_id
        return remote(
            weight_src(piece), weight_dst(tp, piece),
            out_send.at[kind // 2, step - 1], far_recv.at[stage, step - 1],
            (sp, lax.rem(yi + step, pairs) * 2 + half_c),
        )

    def pair_slot(step):
        return lax.rem(yi + step, pairs) * 2 + half_c

    def far_arrival(stage, step):
        block = stage_ref(pair_slot(step), stage)
        return remote(
            block, block, out_send.at[0, 0], far_recv.at[stage, pairs - step - 1], (sp, mate)
        )

    def stage_mate(stage, step):
        block = stage_ref(pair_slot(step), stage)
        return remote(
            block, block, relay_send.at[int(stage >= ROW_CUTS), step - 1],
            relay_recv.at[stage, step - 1], (sp, mate),
        )

    def relay_arrival(stage, step):
        block = stage_ref(lax.rem(yi + step, pairs) * 2 + 1 - half_c, stage)
        return remote(
            block, block, relay_send.at[0, 0], relay_recv.at[stage, step - 1], (sp, mate)
        )

    def relay(stage):
        for step in range(1, pairs):
            far_arrival(stage, step).wait_recv()
            stage_mate(stage, step).start()

    def from_mate(stage):
        for step in range(1, pairs):
            relay_arrival(stage, step).wait_recv()

    own_weights = [
        (rg_hbm, w_gu.at[tp, :, pl.ds(0, fe)], 0),
        (ru_hbm, w_gu.at[tp, :, pl.ds(fe, fe)], 0),
        (rd_hbm, w_d.at[tp], 1),
    ]
    halo_copy = remote(
        rec_in.at[pl.ds(length - 8, 8)], halo, halo_sem.at[0], halo_sem.at[1],
        (lax.rem(sp + 1, sp_n), tp),
    )
    pl.semaphore_wait(barrier, sp_n - 1 + tp_n - 1)
    order = [0, 1, gate_pieces, *range(2, gate_pieces), *range(gate_pieces + 1, len(pieces))]

    def send_weights(piece):
        for step in range(1, pairs):
            weight_out(piece, step).start()

    for place, least in enumerate(EARLY):
        pl.when(zi >= least)(functools.partial(send_weights, order[place]))
    loads[0].wait()

    @pl.when(sp + 1 < sp_n)
    def _():
        halo_copy.start()

    out_w_load = pltpu.make_async_copy(out_w_hbm, out_w, local_sem.at[0])
    out_w_load.start()
    for src, dst, down in own_weights:
        remote(src, dst, own_send.at[down], own_recv.at[down], (sp, mate)).start()
        pltpu.make_async_copy(src, dst, local_sem.at[1 + down]).start()
    shared_loads = [
        pltpu.make_async_copy(sg_hbm, s_gu.at[:, pl.ds(0, fs)], local_sem.at[3]),
        pltpu.make_async_copy(su_hbm, s_gu.at[:, pl.ds(fs, fs)], local_sem.at[4]),
        pltpu.make_async_copy(sd_hbm, s_d, local_sem.at[5]),
    ]
    for load in shared_loads:
        load.start()
    for load in loads[1:]:
        load.wait()

    expert = lax.broadcasted_iota(jnp.int32, (wdense.shape[0], length), 0)
    table = jnp.zeros((wdense.shape[0], length), F32)
    for k in range(ids.shape[0]):
        table = table + jnp.where(expert == ids[k : k + 1], wts[k : k + 1], 0.0)
    wdense[...] = table
    w_in[sp] = table

    def w_out(step):
        return remote(
            wdense, w_in.at[sp], w_send.at[0], w_recv.at[0], (lax.rem(sp + step, sp_n), tp)
        )

    small_blocks, large_blocks = lane_blocks(small_maps), lane_blocks(large_maps)
    rate_rows = -8.0 * softplus(-channel_decay[...])
    rate = jnp.concatenate([rate_rows[0:1], rate_rows[1:2]], axis=1)
    tap_rows = [
        jnp.concatenate([taps[k, 0:1], taps[k, 1:2]], axis=1).astype(F32)
        for k in range(taps.shape[0])
    ]

    padded[pl.ds(8, length)] = rec_in[...].astype(F32).reshape(length, chans)

    @pl.when(sp == 0)
    def _():
        padded[pl.ds(0, 8)] = jnp.zeros((8, chans), F32)

    @pl.when(sp > 0)
    def _():
        halo_copy.wait_recv()
        padded[pl.ds(0, 8)] = halo[...].astype(F32).reshape(8, chans)

    tap_n = taps.shape[0]
    summed = tap_rows[0] * padded[pl.ds(8 - tap_n + 1, length)]
    for k in range(1, tap_n):
        summed = summed + tap_rows[k] * padded[pl.ds(8 - tap_n + 1 + k, length)]
    conv = summed.astype(BF16)
    outs = [
        dot(conv[:, i * LANES : (i + 1) * LANES], maps)
        for i, maps in enumerate(small_blocks + large_blocks)
    ]
    recur = jax.nn.sigmoid(jnp.concatenate([o[:, :LANES] for o in outs], axis=1))
    inp = jax.nn.sigmoid(jnp.concatenate([o[:, LANES:] for o in outs], axis=1))
    log_decay = recur * rate + extra[...].reshape(length, chans)
    decay = jnp.exp(log_decay)
    state = jnp.sqrt(-expm1_negative(2.0 * log_decay)) * inp * conv.astype(F32)
    row_id = lax.broadcasted_iota(jnp.int32, (length, chans), 0)
    shift = 1
    while shift < length:
        live = row_id >= shift
        before_a = jnp.where(live, pltpu.roll(decay, shift, 0), 1.0)
        before_b = jnp.where(live, pltpu.roll(state, shift, 0), 0.0)
        state = decay * before_b + state
        decay = decay * before_a
        shift *= 2
    carry_own[...] = jnp.concatenate(
        [decay[length - 1 :], state[length - 1 :]], axis=0
    )

    def carry_out(step):
        return remote(
            carry_own, carry_in.at[sp], carry_send.at[step], carry_recv.at[sp],
            (lax.rem(sp + step, sp_n), tp),
        )

    def carry_arrival(who):
        return remote(
            carry_own, carry_in.at[who], carry_send.at[0], carry_recv.at[who], (sp, tp)
        )

    @pl.loop(1, sp_n)
    def _(back):
        step = sp_n - back

        @pl.when(sp + step < sp_n)
        def _():
            carry_out(step).start()

    @pl.loop(1, sp_n)
    def _(step):
        w_out(step).start()

    gi = gate_in[...].astype(F32).reshape(length, chans)
    gelu = 0.5 * gi * (1.0 + jnp.tanh(0.7978845608028654 * (gi + 0.044715 * gi * gi * gi)))

    def fold(who, incoming):
        carry_arrival(who).wait_recv()
        link = carry_in[who]
        return link[0:1] * incoming + link[1:2]

    incoming = lax.fori_loop(0, sp, fold, jnp.zeros((1, chans), F32))
    branch = (gelu * (state + decay * incoming)).astype(BF16)
    out_w_load.wait()
    part[...] = dot(branch, out_w[...]).astype(BF16).reshape(part.shape)

    def pair_copy(step):
        slot = lax.rem(yi + step, pairs) * 2 + 1 - half_c
        return remote(
            part.at[slot], pair_in.at[step], pair_send.at[0], pair_recv.at[step], (sp, mate)
        )

    def part_out(step):
        to = lax.rem(yi + step, pairs)
        return remote(
            pair_out.at[step], part_in.at[yi], tp_send.at[step - 1], tp_recv.at[step - 1],
            (sp, to * 2 + half_c),
        )

    def part_arrival(step):
        who = lax.rem(yi + step, pairs)
        return remote(
            pair_out.at[0], part_in.at[who], tp_send.at[0], tp_recv.at[pairs - step - 1], (sp, mate)
        )

    for step in range(1, pairs + 1):
        pair_copy(step % pairs).start()
    for step in range(1, pairs):
        pair_copy(step).wait_recv()
        pair_out[step] = (
            part[pair_slot(step)].astype(F32) + pair_in[step].astype(F32)
        ).astype(BF16)
        part_out(step).start()
    for place, least in enumerate(EARLY):
        if least:
            pl.when(zi < least)(functools.partial(send_weights, order[place]))
    for piece in order[len(EARLY) :]:
        send_weights(piece)
    pair_copy(0).wait_recv()
    mixed = part[tp].astype(F32) + pair_in[0].astype(F32)
    for step in range(1, pairs):
        who = lax.rem(yi + step, pairs)
        part_arrival(step).wait_recv()
        mixed = mixed + part_in[who].astype(F32)
    normed = layer_norm(
        RESIDUAL_SCALE * stream[...].astype(F32) + mixed, n1g[...], n1b[...]
    ).astype(BF16)
    rows[xi, zi] = normed

    def row_piece(col, zj, h):
        return rows.at[col, zj, :, pl.ds(h * half_w, half_w)]

    def row_copy(zj, h, sems, where):
        piece = row_piece(xi, zj, h)
        return remote(piece, piece, sems, ag_recv.at[zj, h], (where, tp))

    def row_right(zj, h):
        return row_copy(zj, h, right_send.at[zj], (zi + 1) * inner + xi)

    def row_left(zj, h):
        return row_copy(zj, h, left_send.at[zj], (zi - 1) * inner + xi)

    def row_across(zj, h):
        piece = row_piece(xi, zj, h)
        return remote(piece, piece, fw_send.at[0], agx_recv.at[0], (x_peer, tp))

    def row_arrival(zj, h):
        piece = row_piece(xi, zj, h)
        return remote(piece, piece, fw_send.at[0], ag_recv.at[zj, h], (x_peer, tp))

    last = outer - 1

    def goes_right(zj):
        far = jnp.logical_and(zj == 0, zi == last - 1)
        return jnp.logical_and(zi < last, jnp.logical_not(far) if outer > 2 else True)

    def goes_left(zj):
        far = jnp.logical_and(zj == last, zi == 1)
        return jnp.logical_and(zi > 0, jnp.logical_not(far) if outer > 2 else True)

    for h in range(SPLITS):
        @pl.when(zi < last)
        def _():
            row_right(zi, h).start()

        @pl.when(zi > 0)
        def _():
            row_left(zi, h).start()

        row_across(zi, h).start()

    if outer > 2:
        for h in range(SPLITS):
            @pl.when(zi == 0)
            def _():
                row_copy(zi, h, left_send.at[zi], last * inner + xi).start()

            @pl.when(zi == last)
            def _():
                row_copy(zi, h, right_send.at[zi], xi).start()

    for stage in (0, ROW_CUTS):
        relay(stage)

    def pass_on(step):
        for h in range(SPLITS):
            @pl.when(zi - step >= 0)
            def _():
                row_arrival(zi - step, h).wait_recv()

                @pl.when(goes_right(zi - step))
                def _():
                    row_right(zi - step, h).start()

                row_across(zi - step, h).start()

            @pl.when(zi + step < outer)
            def _():
                row_arrival(zi + step, h).wait_recv()

                @pl.when(goes_left(zi + step))
                def _():
                    row_left(zi + step, h).start()

                row_across(zi + step, h).start()

    for stage in range(1, ROW_CUTS - 1):
        if stage < outer:
            pass_on(stage)
        relay(stage)

    @pl.loop(ROW_CUTS - 1, outer)
    def _(step):
        pass_on(step)

    for load in shared_loads:
        load.wait()
    up = dot(normed, s_gu[...])
    s_hid = (silu(up[:, :fs]) * up[:, fs:]).astype(BF16)
    moe[...] = dot(s_hid, s_d[...]) + RESIDUAL_SCALE * normed.astype(F32)

    tables = w_in.at[pl.ds(0, sp_n - 1)]
    remote(tables, tables, w_send.at[0], w_recv.at[0], (x_peer, tp)).wait_recv()

    own_rows = lax.broadcasted_iota(jnp.int32, (quarter, length), 0) + tp * quarter
    pick = lax.broadcasted_iota(jnp.int32, (quarter, length), 1) == own_rows

    batch = min(outer, 4)
    tall = batch * quarter
    cap = hid_pack.shape[1] // batch

    def token_weights(col, zj, expert_id):
        line = w_in[zj * inner + col, pl.ds(expert_id, 1)]
        weight = jnp.sum(jnp.where(pick, line, 0.0), axis=1, keepdims=True)
        return jnp.broadcast_to(weight, (quarter, LANES))

    @pl.loop(0, outer)
    def _(zj):
        for j in range(inner):
            w_rows[j, zj] = token_weights(j, zj, sp)
        w_peer[zj] = token_weights(xi, zj, x_peer)

    t_row = lax.broadcasted_iota(jnp.int32, (tall, tall), 0)
    t_col = lax.broadcasted_iota(jnp.int32, (tall, tall), 1)
    same = t_row // quarter == t_col // quarter
    earlier = jnp.where(jnp.logical_and(same, t_col < t_row), 1.0, 0.0).astype(BF16)
    slot_base = (t_row // quarter * cap).astype(F32)

    def places(weights):
        chosen = weights > 0.0
        rank = dot(earlier, jnp.where(chosen, 1.0, 0.0).astype(BF16))
        hit = jnp.logical_and(chosen, t_col.astype(F32) == rank + slot_base)
        return jnp.where(hit, 1.0, 0.0).astype(BF16)

    @pl.loop(0, outer // batch)
    def _(i):
        group = pl.ds(i * batch, batch)
        place_out[i] = places(w_rows[other_x, group].reshape(tall, LANES))
        place_in[i] = places(w_peer[group].reshape(tall, LANES))

    for down in (0, 1):
        own = weight_all(tp, down)
        pltpu.make_async_copy(own, own, local_sem.at[1 + down]).wait()
        theirs = weight_all(mate, down)
        remote(theirs, theirs, own_send.at[down], own_recv.at[down], (sp, mate)).wait_recv()

    def gate_up(col, stage):
        final = stage == ROW_CUTS - 1

        @pl.loop(0, outer // batch)
        def _(i):
            block = rows[
                col, pl.ds(i * batch, batch), :, stage * depth : (stage + 1) * depth
            ].reshape(tall, depth)
            for t in range(tp_n):
                gu = dot(block, w_gu[t, stage * depth : (stage + 1) * depth])
                if stage:
                    gu = gu + gu_acc[col, i, :, t * 2 * fe : (t + 1) * 2 * fe]
                if final:
                    act = (silu(gu[:, :fe]) * gu[:, fe:]).astype(BF16)
                    hid[col, i, :, t * fe : (t + 1) * fe] = act
                else:
                    gu_acc[col, i, :, t * 2 * fe : (t + 1) * 2 * fe] = gu

    for stage in range(ROW_CUTS - 1):
        from_mate(stage)
        gate_up(xi, stage)
    relay(ROW_CUTS - 1)
    side = rows.at[other_x]
    remote(side, side, fw_send.at[0], agx_recv.at[0], (x_peer, tp)).wait_recv()
    for stage in range(ROW_CUTS - 1):
        gate_up(other_x, stage)
    from_mate(ROW_CUTS - 1)
    gate_up(other_x, ROW_CUTS - 1)

    @pl.loop(0, outer // batch)
    def _(i):
        packed = lax.dot_general(
            place_out[i], hid[other_x, i], (((0,), (0,)), ((), ())), preferred_element_type=F32
        )
        hid_pack[i] = packed[: batch * cap].astype(BF16)

    gate_up(xi, ROW_CUTS - 1)

    def columns(ref, c):
        return ref.at[:, :, pl.ds(*spans[c])]

    def x_out(c):
        return remote(
            columns(y_out, c), columns(x_in, c), xs_send.at[0], xs_recv.at[c], (x_peer, tp)
        )

    def z_send(c, step):
        zj = lax.rem(zi + step, outer)
        return remote(
            columns(z_out, c).at[zj], columns(z_in, c).at[zi], zs_send.at[0], zs_recv.at[c],
            (zj * inner + xi, tp),
        )

    def down_across(c):
        first, wide = spans[c]

        @pl.loop(0, outer // batch)
        def _(i):
            value = dot(
                hid_pack[i], w_d[:, :, first : first + wide].reshape(tp_n * fe, wide)
            )
            y_out[i, :, first : first + wide] = value.astype(BF16)

    def down_own(c):
        first, wide = spans[c]

        @pl.loop(0, outer // batch)
        def _(i):
            value = dot(
                hid[xi, i], w_d[:, :, first : first + wide].reshape(tp_n * fe, wide)
            )
            weight = w_rows[xi, pl.ds(i * batch, batch)].reshape(tall, LANES)
            for a in range(0, wide, LANES):
                y_own[pl.ds(i * batch, batch), :, first + a : first + a + LANES] = (
                    (weight * value[:, a : a + LANES]).reshape(batch, quarter, LANES)
                )

    def merge(c):
        first, wide = spans[c]
        at = slice(first, first + wide)
        x_out(c).wait_recv()

        @pl.loop(0, outer // batch)
        def _(i):
            group = pl.ds(i * batch, batch)
            value = dot(place_in[i][:, : batch * cap], x_in[i, :, at])
            weight = w_peer[group].reshape(tall, LANES)
            for a in range(0, wide, LANES):
                cols = slice(first + a, first + a + LANES)
                z_out[group, :, cols] = (
                    y_own[group, :, cols]
                    + (weight * value[:, a : a + LANES]).reshape(batch, quarter, LANES)
                ).astype(BF16)

        @pl.loop(1, outer)
        def _(step):
            z_send(c, step).start()

        moe[:, at] = moe[:, at] + z_out[zi, :, at].astype(F32)

    chunks = len(spans)
    for c in range(chunks):
        if c + 1 < chunks:
            relay(ROW_CUTS + c + 1)
        from_mate(ROW_CUTS + c)
        down_across(c)
        x_out(c).start()
        down_own(c)
        if c >= 2:
            merge(c - 2)
    merge(chunks - 2)
    merge(chunks - 1)

    for c in range(chunks):
        first, wide = spans[c]
        at = slice(first, first + wide)
        group = columns(z_in, c).at[pl.ds(0, outer - 1)]
        remote(group, group, zs_send.at[0], zs_recv.at[c], (x_peer, tp)).wait_recv()

        @pl.loop(1, outer)
        def _(step):
            moe[:, at] += z_in[lax.rem(zi + step, outer), :, at].astype(F32)

    result[...] = layer_norm(moe[...], n2g[...], n2b[...]).astype(BF16)

    for down in (0, 1):
        whole = weight_all(tp, down)
        for step in range(1, pairs):
            remote(whole, whole, out_send.at[down, step - 1], own_recv.at[0], (sp, mate)).wait_send()
            remote(
                whole, whole, relay_send.at[down, step - 1], own_recv.at[0], (sp, mate)
            ).wait_send()
        remote(whole, whole, own_send.at[down], own_recv.at[0], (sp, mate)).wait_send()
    remote(pair_in, pair_in, pair_send.at[0], pair_recv.at[0], (sp, mate)).wait_send()
    for step in range(1, pairs):
        part_out(step).wait_send()
    remote(tables, tables, w_send.at[0], w_recv.at[0], (x_peer, tp)).wait_send()

    @pl.loop(1, sp_n)
    def _(step):
        @pl.when(sp + step < sp_n)
        def _():
            carry_out(step).wait_send()

    @pl.when(sp + 1 < sp_n)
    def _():
        halo_copy.wait_send()

    @pl.loop(0, outer)
    def _(zj):
        block = rows.at[xi, zj]

        ends = jnp.logical_and(zj == zi, outer > 2)

        @pl.when(
            jnp.logical_or(
                jnp.logical_and(zj <= zi, goes_right(zj)), jnp.logical_and(ends, zi == last)
            )
        )
        def _():
            remote(block, block, right_send.at[zj], fw_send.at[0], (x_peer, tp)).wait_send()

        @pl.when(
            jnp.logical_or(
                jnp.logical_and(zj >= zi, goes_left(zj)), jnp.logical_and(ends, zi == 0)
            )
        )
        def _():
            remote(block, block, left_send.at[zj], fw_send.at[0], (x_peer, tp)).wait_send()

    remote(side, side, fw_send.at[0], agx_recv.at[0], (x_peer, tp)).wait_send()
    remote(y_out, y_out, xs_send.at[0], agx_recv.at[0], (x_peer, tp)).wait_send()
    sent = z_out.at[pl.ds(0, outer - 1)]
    remote(sent, sent, zs_send.at[0], agx_recv.at[0], (x_peer, tp)).wait_send()


def shards(
    dims,
    stream,
    recurrence_input,
    output_gate_input,
    convolution_taps,
    first_group_gates,
    second_group_gates,
    channel_decay,
    position_log_extra,
    recurrence_output_weight,
    first_norm_gain,
    first_norm_bias,
    routed_expert_index,
    routed_expert_weight,
    routed_gate_weight,
    routed_up_weight,
    routed_down_weight,
    shared_gate_weight,
    shared_up_weight,
    shared_down_weight,
    second_norm_gain,
    second_norm_bias,
):
    sp_n, tp_n, inner = dims
    outer = sp_n // inner
    length = recurrence_input.shape[0]
    chans = 2 * recurrence_input.shape[2]
    quarter, width = stream.shape
    fe = routed_gate_weight.shape[2]
    fs = shared_gate_weight.shape[1]
    vec = lambda a: a.reshape(1, width)
    vmem = pl.BlockSpec(memory_space=pltpu.VMEM)
    hbm = pl.BlockSpec(memory_space=pltpu.HBM)
    dma = pltpu.SemaphoreType.DMA
    block = (quarter, width)
    pairs = tp_n // 2
    stages = ROW_CUTS + len(COLUMN_CUTS)
    batch = min(outer, 4)
    tall = batch * quarter
    cap = 5 * quarter * routed_expert_index.shape[1] // (4 * sp_n)
    operands = (
        stream,
        recurrence_input,
        output_gate_input,
        convolution_taps,
        first_group_gates,
        second_group_gates,
        channel_decay,
        position_log_extra,
        vec(first_norm_gain),
        vec(first_norm_bias),
        vec(second_norm_gain),
        vec(second_norm_bias),
        routed_expert_index.T,
        routed_expert_weight.T,
    )
    weights = (
        recurrence_output_weight.reshape(chans, width),
        routed_gate_weight.reshape(width, fe),
        routed_up_weight.reshape(width, fe),
        routed_down_weight.reshape(fe, width),
        shared_gate_weight,
        shared_up_weight,
        shared_down_weight,
    )
    limit = (28 + sp_n // 2) * 2**20
    operands = tuple(pltpu.with_memory_space_constraint(a, pltpu.HBM) for a in operands)
    weights = tuple(pltpu.with_memory_space_constraint(a, pltpu.HBM) for a in weights)
    return pl.pallas_call(
        functools.partial(kernel, dims),
        out_shape=jax.ShapeDtypeStruct(block, BF16),
        in_specs=[hbm] * (len(operands) + len(weights)),
        out_specs=vmem,
        scratch_shapes=[
            *(pltpu.VMEM(a.shape, a.dtype) for a in operands),
            dma((len(operands),)),
            pltpu.VMEM((length + 8, chans), F32),
            pltpu.VMEM((8,) + recurrence_input.shape[1:], BF16),
            pltpu.VMEM((2, chans), F32),
            pltpu.VMEM((sp_n, 2, chans), F32),
            pltpu.VMEM((sp_n, length), F32),
            pltpu.VMEM((sp_n, sp_n, length), F32),
            pltpu.VMEM((inner, outer, quarter, LANES), F32),
            pltpu.VMEM((outer, quarter, LANES), F32),
            pltpu.VMEM((outer // batch, tall, LANES), BF16),
            pltpu.VMEM((outer // batch, tall, LANES), BF16),
            pltpu.VMEM((chans, width), BF16),
            pltpu.VMEM((tp_n, width, 2 * fe), BF16),
            pltpu.VMEM((tp_n, fe, width), BF16),
            pltpu.VMEM((width, 2 * fs), BF16),
            pltpu.VMEM((fs, width), BF16),
            pltpu.VMEM((tp_n,) + block, BF16),
            pltpu.VMEM((pairs,) + block, BF16),
            pltpu.VMEM((pairs,) + block, BF16),
            pltpu.VMEM((pairs,) + block, BF16),
            pltpu.VMEM((inner, outer) + block, BF16),
            pltpu.VMEM((inner, outer // batch, tall, tp_n * fe), BF16),
            pltpu.VMEM((outer // batch, batch * cap, tp_n * fe), BF16),
            pltpu.VMEM((inner, outer // batch, batch * quarter, tp_n * 2 * fe), F32),
            pltpu.VMEM((outer,) + block, F32),
            pltpu.VMEM((outer // batch, batch * cap, width), BF16),
            pltpu.VMEM((outer // batch, batch * cap, width), BF16),
            pltpu.VMEM((outer,) + block, BF16),
            pltpu.VMEM((outer,) + block, BF16),
            pltpu.VMEM(block, F32),
            dma((6,)),
            dma((2,)),
            dma((sp_n,)),
            dma((sp_n,)),
            dma((1,)),
            dma((1,)),
            dma((2, pairs - 1)),
            dma((2,)),
            dma((2, pairs - 1)),
            dma((2,)),
            dma((stages, pairs - 1)),
            dma((stages, pairs - 1)),
            dma((1,)),
            dma((pairs,)),
            dma((pairs - 1,)),
            dma((pairs - 1,)),
            dma((outer,)),
            dma((outer,)),
            dma((1,)),
            dma((outer, SPLITS)),
            dma((1,)),
            dma((1,)),
            dma((len(COLUMN_CUTS),)),
            dma((1,)),
            dma((len(COLUMN_CUTS),)),
        ],
        compiler_params=pltpu.CompilerParams(
            has_side_effects=True, collective_id=0, vmem_limit_bytes=limit
        ),
    )(*operands, *weights)


def solution(mesh):
    in_specs = (
        P(("sp", "tp"), None),
        P("sp", None, "tp"),
        P("sp", None, "tp"),
        P(None, None, "tp"),
        P(None, "tp", None, None),
        P(None, "tp", None, None),
        P(None, "tp"),
        P("sp", None, "tp"),
        P(None, "tp", None),
        P(),
        P(),
        P("sp", None),
        P("sp", None),
        P("sp", None, "tp"),
        P("sp", None, "tp"),
        P("sp", "tp", None),
        P(),
        P(),
        P(),
        P(),
        P(),
    )
    dims = (mesh.shape["sp"], mesh.shape["tp"], 2)
    return jax.shard_map(
        functools.partial(shards, dims),
        mesh=mesh,
        in_specs=in_specs,
        out_specs=P(("sp", "tp"), None),
        check_vma=False,
    )
```

```python
import functools

import jax
import jax.numpy as jnp
from jax import lax
from jax.experimental import pallas as pl
from jax.experimental.pallas import tpu as pltpu
from jax.sharding import PartitionSpec as P

RESIDUAL_SCALE = 8.0**0.25
NORM_EPSILON = 1e-05
LANES = 128
ROW_CUTS = 4
COLUMN_CUTS = (2, 2, 2, 2, 2, 2, 2, 2)
EARLY = (0, 0, 1, 2)
SPLITS = 2
MESH = pl.DeviceIdType.MESH
F32 = jnp.float32
BF16 = jnp.bfloat16


def layer_norm(values, gain, bias):
    row_mean = jnp.mean(values, axis=-1, keepdims=True)
    spread = jnp.mean(jnp.square(values - row_mean), axis=-1, keepdims=True)
    return (values - row_mean) * lax.rsqrt(spread + NORM_EPSILON) * gain + bias


def expm1_negative(z):
    small = jnp.full_like(z, 1.0 / 40320.0)
    for n in (5040.0, 720.0, 120.0, 24.0, 6.0, 2.0, 1.0):
        small = small * z + 1.0 / n
    return jnp.where(z > -0.5, small * z, jnp.exp(z) - 1.0)


def softplus(y):
    u = jnp.exp(-jnp.abs(y))
    s = u / (2.0 + u)
    sq = s * s
    series = jnp.full_like(s, 1.0 / 17.0)
    for n in (15.0, 13.0, 11.0, 9.0, 7.0, 5.0, 3.0, 1.0):
        series = series * sq + 1.0 / n
    return jnp.maximum(y, 0.0) + 2.0 * s * series


def lane_blocks(maps_ref):
    kinds, heads, size, _ = maps_ref.shape
    per = LANES // size
    blocks = []
    for start in range(0, heads, per):
        sides = []
        for kind in range(kinds):
            if per == 1:
                sides.append(maps_ref[kind, start])
                continue
            tall = []
            for p in range(per):
                row = lax.broadcasted_iota(jnp.int32, (size, LANES), 0)
                col = lax.broadcasted_iota(jnp.int32, (size, LANES), 1)
                place = jnp.where(col == row + p * size, 1.0, 0.0).astype(BF16)
                tall.append(dot(maps_ref[kind, start + p], place))
            sides.append(jnp.concatenate(tall, axis=0).astype(BF16))
        blocks.append(jnp.concatenate(sides, axis=1))
    return blocks


def silu(v):
    return v * jax.nn.sigmoid(v)


def dot(a, b):
    return jnp.dot(a, b, preferred_element_type=F32)


def kernel(
    dims,
    stream_hbm, rec_hbm, gate_hbm, taps_hbm, small_hbm, large_hbm, decay_hbm, extra_hbm,
    n1g_hbm, n1b_hbm, n2g_hbm, n2b_hbm, ids_hbm, wts_hbm,
    out_w_hbm, rg_hbm, ru_hbm, rd_hbm, sg_hbm, su_hbm, sd_hbm,
    result,
    stream, rec_in, gate_in, taps, small_maps, large_maps, channel_decay, extra, n1g, n1b, n2g, n2b,
    ids, wts, in_sem,
    padded, halo, scan_a, scan_b, carry_own, carry_in, wdense, w_in, w_rows, w_peer, place_out, place_in, out_w, w_gu, w_d, s_gu, s_d,
    part, pair_in, pair_out, part_in, rows, hid, hid_pack, gu_acc, y_own, y_out, x_in, z_out, z_in, moe,
    local_sem, halo_sem, carry_send, carry_recv, w_send, w_recv,
    out_send, own_send, relay_send, own_recv, far_recv, relay_recv, pair_send, pair_recv,
    tp_send, tp_recv, fw_send, ag_recv, agx_recv, xs_send, zs_send,
):
    sp_n, tp_n, inner = dims
    outer = sp_n // inner
    pairs = tp_n // 2
    sp, tp = lax.axis_index("sp"), lax.axis_index("tp")
    zi, xi = sp // inner, lax.rem(sp, inner)
    other_x = lax.rem(xi + 1, inner)
    x_peer = zi * inner + other_x
    half_c = lax.rem(tp, 2)
    yi = tp // 2
    mate = yi * 2 + (1 - half_c)
    length = rec_in.shape[0]
    chans = rec_in.shape[1] * rec_in.shape[2]
    quarter, width = stream.shape
    fe = rg_hbm.shape[1]
    fs = sg_hbm.shape[1]
    unit = width // sum(COLUMN_CUTS)
    spans = []
    for c in range(len(COLUMN_CUTS)):
        spans.append((sum(COLUMN_CUTS[:c]) * unit, COLUMN_CUTS[c] * unit))
    half_w = width // SPLITS

    xs_recv, zs_recv = in_sem, carry_recv
    right_send, left_send = carry_send.at[pl.ds(0, outer)], carry_send.at[pl.ds(outer, outer)]

    def remote(src, dst, send, recv, where):
        return pltpu.make_async_remote_copy(
            src_ref=src, dst_ref=dst, send_sem=send, recv_sem=recv,
            device_id=where, device_id_type=MESH,
        )

    barrier = pltpu.get_barrier_semaphore()
    for step in range(1, tp_n):
        pl.semaphore_signal(
            barrier, inc=1, device_id=(sp, lax.rem(tp + step, tp_n)), device_id_type=MESH
        )

    @pl.loop(1, sp_n)
    def _(step):
        pl.semaphore_signal(
            barrier, inc=1, device_id=(lax.rem(sp + step, sp_n), tp), device_id_type=MESH
        )

    loads = [
        pltpu.make_async_copy(src, dst, in_sem.at[i])
        for i, (src, dst) in enumerate([
            (rec_hbm, rec_in), (small_hbm, small_maps), (large_hbm, large_maps), (taps_hbm, taps),
            (decay_hbm, channel_decay), (extra_hbm, extra), (gate_hbm, gate_in), (ids_hbm, ids),
            (wts_hbm, wts), (stream_hbm, stream), (n1g_hbm, n1g), (n1b_hbm, n1b), (n2g_hbm, n2g),
            (n2b_hbm, n2b),
        ])
    ]
    for load in loads:
        load.start()

    depth = rg_hbm.shape[0] // ROW_CUTS
    pieces = [(kind, part_id) for part_id in range(ROW_CUTS) for kind in (0, 1)]
    gate_pieces = len(pieces)
    pieces += [(2, part_id) for part_id in range(len(spans))]

    def weight_src(piece):
        kind, part_id = pieces[piece]
        if kind == 2:
            return rd_hbm.at[:, pl.ds(*spans[part_id])]
        return (rg_hbm, ru_hbm)[kind].at[pl.ds(part_id * depth, depth)]

    def weight_dst(slot, piece):
        kind, part_id = pieces[piece]
        if kind == 2:
            return w_d.at[slot, :, pl.ds(*spans[part_id])]
        return w_gu.at[slot, pl.ds(part_id * depth, depth), pl.ds(kind * fe, fe)]

    def stage_ref(slot, stage):
        if stage < ROW_CUTS:
            return w_gu.at[slot, pl.ds(stage * depth, depth)]
        return w_d.at[slot, :, pl.ds(*spans[stage - ROW_CUTS])]

    def weight_all(slot, down):
        return (w_d if down else w_gu).at[slot]

    def weight_out(piece, step):
        kind, part_id = pieces[piece]
        stage = ROW_CUTS + part_id if kind == 2 else part_id
        return remote(
            weight_src(piece), weight_dst(tp, piece),
            out_send.at[kind // 2, step - 1], far_recv.at[stage, step - 1],
            (sp, lax.rem(yi + step, pairs) * 2 + half_c),
        )

    def pair_slot(step):
        return lax.rem(yi + step, pairs) * 2 + half_c

    def far_arrival(stage, step):
        block = stage_ref(pair_slot(step), stage)
        return remote(
            block, block, out_send.at[0, 0], far_recv.at[stage, pairs - step - 1], (sp, mate)
        )

    def stage_mate(stage, step):
        block = stage_ref(pair_slot(step), stage)
        return remote(
            block, block, relay_send.at[int(stage >= ROW_CUTS), step - 1],
            relay_recv.at[stage, step - 1], (sp, mate),
        )

    def relay_arrival(stage, step):
        block = stage_ref(lax.rem(yi + step, pairs) * 2 + 1 - half_c, stage)
        return remote(
            block, block, relay_send.at[0, 0], relay_recv.at[stage, step - 1], (sp, mate)
        )

    def relay(stage):
        for step in range(1, pairs):
            far_arrival(stage, step).wait_recv()
            stage_mate(stage, step).start()

    def from_mate(stage):
        for step in range(1, pairs):
            relay_arrival(stage, step).wait_recv()

    own_weights = [
        (rg_hbm, w_gu.at[tp, :, pl.ds(0, fe)], 0),
        (ru_hbm, w_gu.at[tp, :, pl.ds(fe, fe)], 0),
        (rd_hbm, w_d.at[tp], 1),
    ]
    halo_copy = remote(
        rec_in.at[pl.ds(length - 8, 8)], halo, halo_sem.at[0], halo_sem.at[1],
        (lax.rem(sp + 1, sp_n), tp),
    )
    pl.semaphore_wait(barrier, sp_n - 1 + tp_n - 1)
    order = [0, gate_pieces, *range(1, gate_pieces), *range(gate_pieces + 1, len(pieces))]

    def send_weights(piece):
        for step in range(1, pairs):
            weight_out(piece, step).start()

    for place, least in enumerate(EARLY):
        pl.when(sp >= least)(functools.partial(send_weights, order[place]))
    loads[0].wait()

    @pl.when(sp + 1 < sp_n)
    def _():
        halo_copy.start()

    out_w_load = pltpu.make_async_copy(out_w_hbm, out_w, local_sem.at[0])
    out_w_load.start()
    for src, dst, down in own_weights:
        remote(src, dst, own_send.at[down], own_recv.at[down], (sp, mate)).start()
        pltpu.make_async_copy(src, dst, local_sem.at[1 + down]).start()
    shared_loads = [
        pltpu.make_async_copy(sg_hbm, s_gu.at[:, pl.ds(0, fs)], local_sem.at[3]),
        pltpu.make_async_copy(su_hbm, s_gu.at[:, pl.ds(fs, fs)], local_sem.at[4]),
        pltpu.make_async_copy(sd_hbm, s_d, local_sem.at[5]),
    ]
    for load in shared_loads:
        load.start()
    for load in loads[1:]:
        load.wait()

    expert = lax.broadcasted_iota(jnp.int32, (wdense.shape[0], length), 0)
    table = jnp.zeros((wdense.shape[0], length), F32)
    for k in range(ids.shape[0]):
        table = table + jnp.where(expert == ids[k : k + 1], wts[k : k + 1], 0.0)
    wdense[...] = table
    w_in[sp] = table

    def w_out(step):
        return remote(
            wdense, w_in.at[sp], w_send.at[0], w_recv.at[0], (lax.rem(sp + step, sp_n), tp)
        )

    small_blocks, large_blocks = lane_blocks(small_maps), lane_blocks(large_maps)
    rate_rows = -8.0 * softplus(-channel_decay[...])
    rate = jnp.concatenate([rate_rows[0:1], rate_rows[1:2]], axis=1)
    tap_rows = [
        jnp.concatenate([taps[k, 0:1], taps[k, 1:2]], axis=1).astype(F32)
        for k in range(taps.shape[0])
    ]

    padded[pl.ds(8, length)] = rec_in[...].astype(F32).reshape(length, chans)
    tap_n = taps.shape[0]

    def segment(first, count):
        base = 8 + first - tap_n + 1
        summed = tap_rows[0] * padded[pl.ds(base, count)]
        for k in range(1, tap_n):
            summed = summed + tap_rows[k] * padded[pl.ds(base + k, count)]
        conv = summed.astype(BF16)
        outs = [
            dot(conv[:, i * LANES : (i + 1) * LANES], maps)
            for i, maps in enumerate(small_blocks + large_blocks)
        ]
        recur = jax.nn.sigmoid(jnp.concatenate([o[:, :LANES] for o in outs], axis=1))
        inp = jax.nn.sigmoid(jnp.concatenate([o[:, LANES:] for o in outs], axis=1))
        log_decay = recur * rate + extra[pl.ds(first, count)].reshape(count, chans)
        decay = jnp.exp(log_decay)
        state = jnp.sqrt(-expm1_negative(2.0 * log_decay)) * inp * conv.astype(F32)
        row_id = lax.broadcasted_iota(jnp.int32, (count, chans), 0)
        shift = 1
        while shift < count:
            live = row_id >= shift
            before_a = jnp.where(live, pltpu.roll(decay, shift, 0), 1.0)
            before_b = jnp.where(live, pltpu.roll(state, shift, 0), 0.0)
            state = decay * before_b + state
            decay = decay * before_a
            shift *= 2
        return decay, state

    decay_b, state_b = segment(8, length - 8)
    scan_a[...] = decay_b
    scan_b[...] = state_b

    @pl.when(sp == 0)
    def _():
        padded[pl.ds(0, 8)] = jnp.zeros((8, chans), F32)

    @pl.when(sp > 0)
    def _():
        halo_copy.wait_recv()
        padded[pl.ds(0, 8)] = halo[...].astype(F32).reshape(8, chans)

    decay_a, state_a = segment(0, 8)
    end_a, end_b = scan_a[length - 9 :], scan_b[length - 9 :]
    carry_own[...] = jnp.concatenate(
        [end_a * decay_a[7:], end_a * state_a[7:] + end_b], axis=0
    )

    def carry_out(step):
        return remote(
            carry_own, carry_in.at[sp], carry_send.at[step], carry_recv.at[sp],
            (lax.rem(sp + step, sp_n), tp),
        )

    def carry_arrival(who):
        return remote(
            carry_own, carry_in.at[who], carry_send.at[0], carry_recv.at[who], (sp, tp)
        )

    @pl.loop(1, sp_n)
    def _(back):
        step = sp_n - back

        @pl.when(sp + step < sp_n)
        def _():
            carry_out(step).start()

    @pl.loop(1, sp_n)
    def _(step):
        w_out(step).start()

    gi = gate_in[...].astype(F32).reshape(length, chans)
    gelu = 0.5 * gi * (1.0 + jnp.tanh(0.7978845608028654 * (gi + 0.044715 * gi * gi * gi)))

    def fold(who, incoming):
        carry_arrival(who).wait_recv()
        link = carry_in[who]
        return link[0:1] * incoming + link[1:2]

    incoming = lax.fori_loop(0, sp, fold, jnp.zeros((1, chans), F32))
    head = state_a + decay_a * incoming
    rest = scan_b[...] + scan_a[...] * head[7:]
    branch = (gelu * jnp.concatenate([head, rest], axis=0)).astype(BF16)
    out_w_load.wait()
    part[...] = dot(branch, out_w[...]).astype(BF16).reshape(part.shape)

    def pair_copy(step):
        slot = lax.rem(yi + step, pairs) * 2 + 1 - half_c
        return remote(
            part.at[slot], pair_in.at[step], pair_send.at[0], pair_recv.at[step], (sp, mate)
        )

    def part_out(step):
        to = lax.rem(yi + step, pairs)
        return remote(
            pair_out.at[step], part_in.at[yi], tp_send.at[step - 1], tp_recv.at[step - 1],
            (sp, to * 2 + half_c),
        )

    def part_arrival(step):
        who = lax.rem(yi + step, pairs)
        return remote(
            pair_out.at[0], part_in.at[who], tp_send.at[0], tp_recv.at[pairs - step - 1], (sp, mate)
        )

    for step in range(1, pairs + 1):
        pair_copy(step % pairs).start()
    for step in range(1, pairs):
        pair_copy(step).wait_recv()
        pair_out[step] = (
            part[pair_slot(step)].astype(F32) + pair_in[step].astype(F32)
        ).astype(BF16)
        part_out(step).start()
    for place, least in enumerate(EARLY):
        if least:
            pl.when(sp < least)(functools.partial(send_weights, order[place]))
    for piece in order[len(EARLY) :]:
        send_weights(piece)
    @pl.loop(1, sp_n)
    def _(step):
        @pl.when(sp + step < sp_n)
        def _():
            carry_out(step).wait_send()

    pair_copy(0).wait_recv()
    mixed = part[tp].astype(F32) + pair_in[0].astype(F32)
    for step in range(1, pairs):
        who = lax.rem(yi + step, pairs)
        part_arrival(step).wait_recv()
        mixed = mixed + part_in[who].astype(F32)
    normed = layer_norm(
        RESIDUAL_SCALE * stream[...].astype(F32) + mixed, n1g[...], n1b[...]
    ).astype(BF16)
    rows[xi, zi] = normed

    def row_piece(col, zj, h):
        return rows.at[col, zj, :, pl.ds(h * half_w, half_w)]

    def row_copy(zj, h, sems, where):
        piece = row_piece(xi, zj, h)
        return remote(piece, piece, sems, ag_recv.at[zj, h], (where, tp))

    def row_right(zj, h):
        return row_copy(zj, h, right_send.at[zj], (zi + 1) * inner + xi)

    def row_left(zj, h):
        return row_copy(zj, h, left_send.at[zj], (zi - 1) * inner + xi)

    def row_across(zj, h):
        piece = row_piece(xi, zj, h)
        return remote(piece, piece, fw_send.at[0], agx_recv.at[0], (x_peer, tp))

    def row_arrival(zj, h):
        piece = row_piece(xi, zj, h)
        return remote(piece, piece, fw_send.at[0], ag_recv.at[zj, h], (x_peer, tp))

    last = outer - 1

    def goes_right(zj):
        far = jnp.logical_and(zj == 0, zi == last - 1)
        return jnp.logical_and(zi < last, jnp.logical_not(far) if outer > 2 else True)

    def goes_left(zj):
        far = jnp.logical_and(zj == last, zi == 1)
        return jnp.logical_and(zi > 0, jnp.logical_not(far) if outer > 2 else True)

    for h in range(SPLITS):
        @pl.when(zi < last)
        def _():
            row_right(zi, h).start()

        @pl.when(zi > 0)
        def _():
            row_left(zi, h).start()

        row_across(zi, h).start()

    if outer > 2:
        for h in range(SPLITS):
            @pl.when(zi == 0)
            def _():
                row_copy(zi, h, left_send.at[zi], last * inner + xi).start()

            @pl.when(zi == last)
            def _():
                row_copy(zi, h, right_send.at[zi], xi).start()

    for stage in (0, ROW_CUTS):
        relay(stage)

    def pass_on(step):
        for h in range(SPLITS):
            @pl.when(zi - step >= 0)
            def _():
                row_arrival(zi - step, h).wait_recv()

                @pl.when(goes_right(zi - step))
                def _():
                    row_right(zi - step, h).start()

                row_across(zi - step, h).start()

            @pl.when(zi + step < outer)
            def _():
                row_arrival(zi + step, h).wait_recv()

                @pl.when(goes_left(zi + step))
                def _():
                    row_left(zi + step, h).start()

                row_across(zi + step, h).start()

    for stage in range(1, ROW_CUTS - 1):
        if stage < outer:
            pass_on(stage)
        relay(stage)

    @pl.loop(ROW_CUTS - 1, outer)
    def _(step):
        pass_on(step)

    for load in shared_loads:
        load.wait()
    up = dot(normed, s_gu[...])
    s_hid = (silu(up[:, :fs]) * up[:, fs:]).astype(BF16)
    moe[...] = dot(s_hid, s_d[...]) + RESIDUAL_SCALE * normed.astype(F32)

    tables = w_in.at[pl.ds(0, sp_n - 1)]
    remote(tables, tables, w_send.at[0], w_recv.at[0], (x_peer, tp)).wait_recv()

    own_rows = lax.broadcasted_iota(jnp.int32, (quarter, length), 0) + tp * quarter
    pick = lax.broadcasted_iota(jnp.int32, (quarter, length), 1) == own_rows

    batch = min(outer, 4)
    tall = batch * quarter
    cap = hid_pack.shape[1] // batch

    def token_weights(col, zj, expert_id):
        line = w_in[zj * inner + col, pl.ds(expert_id, 1)]
        weight = jnp.sum(jnp.where(pick, line, 0.0), axis=1, keepdims=True)
        return jnp.broadcast_to(weight, (quarter, LANES))

    @pl.loop(0, outer)
    def _(zj):
        for j in range(inner):
            w_rows[j, zj] = token_weights(j, zj, sp)
        w_peer[zj] = token_weights(xi, zj, x_peer)

    t_row = lax.broadcasted_iota(jnp.int32, (tall, tall), 0)
    t_col = lax.broadcasted_iota(jnp.int32, (tall, tall), 1)
    same = t_row // quarter == t_col // quarter
    earlier = jnp.where(jnp.logical_and(same, t_col < t_row), 1.0, 0.0).astype(BF16)
    slot_base = (t_row // quarter * cap).astype(F32)

    def places(weights):
        chosen = weights > 0.0
        rank = dot(earlier, jnp.where(chosen, 1.0, 0.0).astype(BF16))
        hit = jnp.logical_and(chosen, t_col.astype(F32) == rank + slot_base)
        return jnp.where(hit, 1.0, 0.0).astype(BF16)

    @pl.loop(0, outer // batch)
    def _(i):
        group = pl.ds(i * batch, batch)
        place_out[i] = places(w_rows[other_x, group].reshape(tall, LANES))
        place_in[i] = places(w_peer[group].reshape(tall, LANES))

    for down in (0, 1):
        own = weight_all(tp, down)
        pltpu.make_async_copy(own, own, local_sem.at[1 + down]).wait()
        theirs = weight_all(mate, down)
        remote(theirs, theirs, own_send.at[down], own_recv.at[down], (sp, mate)).wait_recv()

    def gate_up(col, stage):
        final = stage == ROW_CUTS - 1

        @pl.loop(0, outer // batch)
        def _(i):
            block = rows[
                col, pl.ds(i * batch, batch), :, stage * depth : (stage + 1) * depth
            ].reshape(tall, depth)
            for t in range(tp_n):
                gu = dot(block, w_gu[t, stage * depth : (stage + 1) * depth])
                if stage:
                    gu = gu + gu_acc[col, i, :, t * 2 * fe : (t + 1) * 2 * fe]
                if final:
                    act = (silu(gu[:, :fe]) * gu[:, fe:]).astype(BF16)
                    hid[col, i, :, t * fe : (t + 1) * fe] = act
                else:
                    gu_acc[col, i, :, t * 2 * fe : (t + 1) * 2 * fe] = gu

    for stage in range(ROW_CUTS - 1):
        from_mate(stage)
        gate_up(xi, stage)
    relay(ROW_CUTS - 1)
    side = rows.at[other_x]
    remote(side, side, fw_send.at[0], agx_recv.at[0], (x_peer, tp)).wait_recv()
    for stage in range(ROW_CUTS - 1):
        gate_up(other_x, stage)
    from_mate(ROW_CUTS - 1)
    gate_up(other_x, ROW_CUTS - 1)

    @pl.loop(0, outer // batch)
    def _(i):
        packed = lax.dot_general(
            place_out[i], hid[other_x, i], (((0,), (0,)), ((), ())), preferred_element_type=F32
        )
        hid_pack[i] = packed[: batch * cap].astype(BF16)

    gate_up(xi, ROW_CUTS - 1)

    def columns(ref, c):
        return ref.at[:, :, pl.ds(*spans[c])]

    def x_out(c):
        return remote(
            columns(y_out, c), columns(x_in, c), xs_send.at[0], xs_recv.at[c], (x_peer, tp)
        )

    def z_target(step):
        down_to, up_to = last + 1 - step, step - 1
        down_to = jnp.where(down_to > zi, down_to, down_to - 1)
        up_to = jnp.where(up_to < zi, up_to, up_to + 1)
        return jnp.where(zi < outer // 2, down_to, up_to)

    def z_send(c, step):
        zj = z_target(step)
        return remote(
            columns(z_out, c).at[zj], columns(z_in, c).at[zi], zs_send.at[0], zs_recv.at[c],
            (zj * inner + xi, tp),
        )

    def down_across(c):
        first, wide = spans[c]

        @pl.loop(0, outer // batch)
        def _(i):
            value = dot(
                hid_pack[i], w_d[:, :, first : first + wide].reshape(tp_n * fe, wide)
            )
            y_out[i, :, first : first + wide] = value.astype(BF16)

    def down_own(c):
        first, wide = spans[c]

        @pl.loop(0, outer // batch)
        def _(i):
            value = dot(
                hid[xi, i], w_d[:, :, first : first + wide].reshape(tp_n * fe, wide)
            )
            weight = w_rows[xi, pl.ds(i * batch, batch)].reshape(tall, LANES)
            for a in range(0, wide, LANES):
                y_own[pl.ds(i * batch, batch), :, first + a : first + a + LANES] = (
                    (weight * value[:, a : a + LANES]).reshape(batch, quarter, LANES)
                )

    def merge(c):
        first, wide = spans[c]
        at = slice(first, first + wide)
        x_out(c).wait_recv()

        @pl.loop(0, outer // batch)
        def _(i):
            group = pl.ds(i * batch, batch)
            value = dot(place_in[i][:, : batch * cap], x_in[i, :, at])
            weight = w_peer[group].reshape(tall, LANES)
            for a in range(0, wide, LANES):
                cols = slice(first + a, first + a + LANES)
                z_out[group, :, cols] = (
                    y_own[group, :, cols]
                    + (weight * value[:, a : a + LANES]).reshape(batch, quarter, LANES)
                ).astype(BF16)

        @pl.loop(1, outer)
        def _(step):
            z_send(c, step).start()

        moe[:, at] = moe[:, at] + z_out[zi, :, at].astype(F32)

    chunks = len(spans)
    for c in range(chunks):
        if c + 1 < chunks:
            relay(ROW_CUTS + c + 1)
        from_mate(ROW_CUTS + c)
        down_across(c)
        x_out(c).start()
        down_own(c)
        if c >= 2:
            merge(c - 2)
    merge(chunks - 2)
    merge(chunks - 1)

    for c in range(chunks):
        first, wide = spans[c]
        at = slice(first, first + wide)
        group = columns(z_in, c).at[pl.ds(0, outer - 1)]
        remote(group, group, zs_send.at[0], zs_recv.at[c], (x_peer, tp)).wait_recv()

        @pl.loop(1, outer)
        def _(step):
            moe[:, at] += z_in[lax.rem(zi + step, outer), :, at].astype(F32)

    result[...] = layer_norm(moe[...], n2g[...], n2b[...]).astype(BF16)

    for down in (0, 1):
        whole = weight_all(tp, down)
        for step in range(1, pairs):
            remote(whole, whole, out_send.at[down, step - 1], own_recv.at[0], (sp, mate)).wait_send()
            remote(
                whole, whole, relay_send.at[down, step - 1], own_recv.at[0], (sp, mate)
            ).wait_send()
        remote(whole, whole, own_send.at[down], own_recv.at[0], (sp, mate)).wait_send()
    remote(pair_in, pair_in, pair_send.at[0], pair_recv.at[0], (sp, mate)).wait_send()
    for step in range(1, pairs):
        part_out(step).wait_send()
    remote(tables, tables, w_send.at[0], w_recv.at[0], (x_peer, tp)).wait_send()

    @pl.when(sp + 1 < sp_n)
    def _():
        halo_copy.wait_send()

    @pl.loop(0, outer)
    def _(zj):
        block = rows.at[xi, zj]

        ends = jnp.logical_and(zj == zi, outer > 2)

        @pl.when(
            jnp.logical_or(
                jnp.logical_and(zj <= zi, goes_right(zj)), jnp.logical_and(ends, zi == last)
            )
        )
        def _():
            remote(block, block, right_send.at[zj], fw_send.at[0], (x_peer, tp)).wait_send()

        @pl.when(
            jnp.logical_or(
                jnp.logical_and(zj >= zi, goes_left(zj)), jnp.logical_and(ends, zi == 0)
            )
        )
        def _():
            remote(block, block, left_send.at[zj], fw_send.at[0], (x_peer, tp)).wait_send()

    remote(side, side, fw_send.at[0], agx_recv.at[0], (x_peer, tp)).wait_send()
    remote(y_out, y_out, xs_send.at[0], agx_recv.at[0], (x_peer, tp)).wait_send()
    sent = z_out.at[pl.ds(0, outer - 1)]
    remote(sent, sent, zs_send.at[0], agx_recv.at[0], (x_peer, tp)).wait_send()


def shards(
    dims,
    stream,
    recurrence_input,
    output_gate_input,
    convolution_taps,
    first_group_gates,
    second_group_gates,
    channel_decay,
    position_log_extra,
    recurrence_output_weight,
    first_norm_gain,
    first_norm_bias,
    routed_expert_index,
    routed_expert_weight,
    routed_gate_weight,
    routed_up_weight,
    routed_down_weight,
    shared_gate_weight,
    shared_up_weight,
    shared_down_weight,
    second_norm_gain,
    second_norm_bias,
):
    sp_n, tp_n, inner = dims
    outer = sp_n // inner
    length = recurrence_input.shape[0]
    chans = 2 * recurrence_input.shape[2]
    quarter, width = stream.shape
    fe = routed_gate_weight.shape[2]
    fs = shared_gate_weight.shape[1]
    vec = lambda a: a.reshape(1, width)
    vmem = pl.BlockSpec(memory_space=pltpu.VMEM)
    hbm = pl.BlockSpec(memory_space=pltpu.HBM)
    dma = pltpu.SemaphoreType.DMA
    block = (quarter, width)
    pairs = tp_n // 2
    stages = ROW_CUTS + len(COLUMN_CUTS)
    batch = min(outer, 4)
    tall = batch * quarter
    cap = 5 * quarter * routed_expert_index.shape[1] // (4 * sp_n)
    operands = (
        stream,
        recurrence_input,
        output_gate_input,
        convolution_taps,
        first_group_gates,
        second_group_gates,
        channel_decay,
        position_log_extra,
        vec(first_norm_gain),
        vec(first_norm_bias),
        vec(second_norm_gain),
        vec(second_norm_bias),
        routed_expert_index.T,
        routed_expert_weight.T,
    )
    weights = (
        recurrence_output_weight.reshape(chans, width),
        routed_gate_weight.reshape(width, fe),
        routed_up_weight.reshape(width, fe),
        routed_down_weight.reshape(fe, width),
        shared_gate_weight,
        shared_up_weight,
        shared_down_weight,
    )
    limit = (28 + sp_n // 2) * 2**20
    operands = tuple(pltpu.with_memory_space_constraint(a, pltpu.HBM) for a in operands)
    weights = tuple(pltpu.with_memory_space_constraint(a, pltpu.HBM) for a in weights)
    return pl.pallas_call(
        functools.partial(kernel, dims),
        out_shape=jax.ShapeDtypeStruct(block, BF16),
        in_specs=[hbm] * (len(operands) + len(weights)),
        out_specs=vmem,
        scratch_shapes=[
            *(pltpu.VMEM(a.shape, a.dtype) for a in operands),
            dma((len(operands),)),
            pltpu.VMEM((length + 8, chans), F32),
            pltpu.VMEM((8,) + recurrence_input.shape[1:], BF16),
            pltpu.VMEM((length - 8, chans), F32),
            pltpu.VMEM((length - 8, chans), F32),
            pltpu.VMEM((2, chans), F32),
            pltpu.VMEM((sp_n, 2, chans), F32),
            pltpu.VMEM((sp_n, length), F32),
            pltpu.VMEM((sp_n, sp_n, length), F32),
            pltpu.VMEM((inner, outer, quarter, LANES), F32),
            pltpu.VMEM((outer, quarter, LANES), F32),
            pltpu.VMEM((outer // batch, tall, LANES), BF16),
            pltpu.VMEM((outer // batch, tall, LANES), BF16),
            pltpu.VMEM((chans, width), BF16),
            pltpu.VMEM((tp_n, width, 2 * fe), BF16),
            pltpu.VMEM((tp_n, fe, width), BF16),
            pltpu.VMEM((width, 2 * fs), BF16),
            pltpu.VMEM((fs, width), BF16),
            pltpu.VMEM((tp_n,) + block, BF16),
            pltpu.VMEM((pairs,) + block, BF16),
            pltpu.VMEM((pairs,) + block, BF16),
            pltpu.VMEM((pairs,) + block, BF16),
            pltpu.VMEM((inner, outer) + block, BF16),
            pltpu.VMEM((inner, outer // batch, tall, tp_n * fe), BF16),
            pltpu.VMEM((outer // batch, batch * cap, tp_n * fe), BF16),
            pltpu.VMEM((inner, outer // batch, batch * quarter, tp_n * 2 * fe), F32),
            pltpu.VMEM((outer,) + block, F32),
            pltpu.VMEM((outer // batch, batch * cap, width), BF16),
            pltpu.VMEM((outer // batch, batch * cap, width), BF16),
            pltpu.VMEM((outer,) + block, BF16),
            pltpu.VMEM((outer,) + block, BF16),
            pltpu.VMEM(block, F32),
            dma((6,)),
            dma((2,)),
            dma((sp_n,)),
            dma((sp_n,)),
            dma((1,)),
            dma((1,)),
            dma((2, pairs - 1)),
            dma((2,)),
            dma((2, pairs - 1)),
            dma((2,)),
            dma((stages, pairs - 1)),
            dma((stages, pairs - 1)),
            dma((1,)),
            dma((pairs,)),
            dma((pairs - 1,)),
            dma((pairs - 1,)),
            dma((1,)),
            dma((outer, SPLITS)),
            dma((1,)),
            dma((1,)),
            dma((1,)),
        ],
        compiler_params=pltpu.CompilerParams(
            has_side_effects=True, collective_id=0, vmem_limit_bytes=limit
        ),
    )(*operands, *weights)


def solution(mesh):
    in_specs = (
        P(("sp", "tp"), None),
        P("sp", None, "tp"),
        P("sp", None, "tp"),
        P(None, None, "tp"),
        P(None, "tp", None, None),
        P(None, "tp", None, None),
        P(None, "tp"),
        P("sp", None, "tp"),
        P(None, "tp", None),
        P(),
        P(),
        P("sp", None),
        P("sp", None),
        P("sp", None, "tp"),
        P("sp", None, "tp"),
        P("sp", "tp", None),
        P(),
        P(),
        P(),
        P(),
        P(),
    )
    dims = (mesh.shape["sp"], mesh.shape["tp"], 2)
    return jax.shard_map(
        functools.partial(shards, dims),
        mesh=mesh,
        in_specs=in_specs,
        out_specs=P(("sp", "tp"), None),
        check_vma=False,
    )
```

```python
import functools

import jax
import jax.numpy as jnp
from jax import lax
from jax.experimental import pallas as pl
from jax.experimental.pallas import tpu as pltpu
from jax.sharding import PartitionSpec as P

RESIDUAL_SCALE = 8.0**0.25
NORM_EPSILON = 1e-05
LANES = 128
ROW_CUTS = 4
COLUMN_CUTS = (2, 2, 2, 2, 2, 2, 2, 2)
EARLY = (0, 0, 1, 2)
SPLITS = 2
MESH = pl.DeviceIdType.MESH
F32 = jnp.float32
BF16 = jnp.bfloat16


def layer_norm(values, gain, bias):
    row_mean = jnp.mean(values, axis=-1, keepdims=True)
    spread = jnp.mean(jnp.square(values - row_mean), axis=-1, keepdims=True)
    return (values - row_mean) * lax.rsqrt(spread + NORM_EPSILON) * gain + bias


def expm1_negative(z):
    small = jnp.full_like(z, 1.0 / 40320.0)
    for n in (5040.0, 720.0, 120.0, 24.0, 6.0, 2.0, 1.0):
        small = small * z + 1.0 / n
    return jnp.where(z > -0.5, small * z, jnp.exp(z) - 1.0)


def softplus(y):
    u = jnp.exp(-jnp.abs(y))
    s = u / (2.0 + u)
    sq = s * s
    series = jnp.full_like(s, 1.0 / 17.0)
    for n in (15.0, 13.0, 11.0, 9.0, 7.0, 5.0, 3.0, 1.0):
        series = series * sq + 1.0 / n
    return jnp.maximum(y, 0.0) + 2.0 * s * series


def lane_blocks(maps_ref):
    kinds, heads, size, _ = maps_ref.shape
    per = LANES // size
    blocks = []
    for start in range(0, heads, per):
        sides = []
        for kind in range(kinds):
            if per == 1:
                sides.append(maps_ref[kind, start])
                continue
            tall = []
            for p in range(per):
                row = lax.broadcasted_iota(jnp.int32, (size, LANES), 0)
                col = lax.broadcasted_iota(jnp.int32, (size, LANES), 1)
                place = jnp.where(col == row + p * size, 1.0, 0.0).astype(BF16)
                tall.append(dot(maps_ref[kind, start + p], place))
            sides.append(jnp.concatenate(tall, axis=0).astype(BF16))
        blocks.append(jnp.concatenate(sides, axis=1))
    return blocks


def silu(v):
    return v * jax.nn.sigmoid(v)


def dot(a, b):
    return jnp.dot(a, b, preferred_element_type=F32)


def kernel(
    dims,
    stream_hbm, rec_hbm, gate_hbm, taps_hbm, small_hbm, large_hbm, decay_hbm, extra_hbm,
    n1g_hbm, n1b_hbm, n2g_hbm, n2b_hbm, ids_hbm, wts_hbm,
    out_w_hbm, rg_hbm, ru_hbm, rd_hbm, sg_hbm, su_hbm, sd_hbm,
    result,
    stream, rec_in, gate_in, taps, small_maps, large_maps, channel_decay, extra, n1g, n1b, n2g, n2b,
    ids, wts, in_sem,
    padded, halo, scan_a, scan_b, carry_own, carry_in, wdense, w_in, w_rows, w_peer, place_out, place_in, out_w, w_gu, w_d, s_gu, s_d,
    part, pair_in, pair_out, part_in, rows, hid, hid_pack, gu_acc, y_own, y_out, x_in, z_out, z_in, moe,
    local_sem, halo_sem, carry_send, carry_recv, w_send, w_recv,
    out_send, own_send, relay_send, own_recv, far_recv, relay_recv, pair_send, pair_recv,
    tp_send, tp_recv, fw_send, ag_recv, agx_recv, xs_send, zs_send,
):
    sp_n, tp_n, inner = dims
    outer = sp_n // inner
    pairs = tp_n // 2
    sp, tp = lax.axis_index("sp"), lax.axis_index("tp")
    zi, xi = sp // inner, lax.rem(sp, inner)
    other_x = lax.rem(xi + 1, inner)
    x_peer = zi * inner + other_x
    half_c = lax.rem(tp, 2)
    yi = tp // 2
    mate = yi * 2 + (1 - half_c)
    length = rec_in.shape[0]
    chans = rec_in.shape[1] * rec_in.shape[2]
    quarter, width = stream.shape
    fe = rg_hbm.shape[1]
    fs = sg_hbm.shape[1]
    unit = width // sum(COLUMN_CUTS)
    spans = []
    for c in range(len(COLUMN_CUTS)):
        spans.append((sum(COLUMN_CUTS[:c]) * unit, COLUMN_CUTS[c] * unit))
    half_w = width // SPLITS

    xs_recv, zs_recv = in_sem, carry_recv
    right_send, left_send = carry_send.at[pl.ds(0, outer)], carry_send.at[pl.ds(outer, outer)]

    def remote(src, dst, send, recv, where):
        return pltpu.make_async_remote_copy(
            src_ref=src, dst_ref=dst, send_sem=send, recv_sem=recv,
            device_id=where, device_id_type=MESH,
        )

    barrier = pltpu.get_barrier_semaphore()
    for step in range(1, tp_n):
        pl.semaphore_signal(
            barrier, inc=1, device_id=(sp, lax.rem(tp + step, tp_n)), device_id_type=MESH
        )

    @pl.loop(1, sp_n)
    def _(step):
        pl.semaphore_signal(
            barrier, inc=1, device_id=(lax.rem(sp + step, sp_n), tp), device_id_type=MESH
        )

    loads = [
        pltpu.make_async_copy(src, dst, in_sem.at[i])
        for i, (src, dst) in enumerate([
            (rec_hbm, rec_in), (small_hbm, small_maps), (large_hbm, large_maps), (taps_hbm, taps),
            (decay_hbm, channel_decay), (extra_hbm, extra), (gate_hbm, gate_in), (ids_hbm, ids),
            (wts_hbm, wts), (stream_hbm, stream), (n1g_hbm, n1g), (n1b_hbm, n1b), (n2g_hbm, n2g),
            (n2b_hbm, n2b),
        ])
    ]
    for load in loads:
        load.start()

    depth = rg_hbm.shape[0] // ROW_CUTS
    pieces = [(kind, part_id) for part_id in range(ROW_CUTS) for kind in (0, 1)]
    gate_pieces = len(pieces)
    pieces += [(2, part_id) for part_id in range(len(spans))]

    def weight_src(piece):
        kind, part_id = pieces[piece]
        if kind == 2:
            return rd_hbm.at[:, pl.ds(*spans[part_id])]
        return (rg_hbm, ru_hbm)[kind].at[pl.ds(part_id * depth, depth)]

    def weight_dst(slot, piece):
        kind, part_id = pieces[piece]
        if kind == 2:
            return w_d.at[slot, :, pl.ds(*spans[part_id])]
        return w_gu.at[slot, pl.ds(part_id * depth, depth), pl.ds(kind * fe, fe)]

    def stage_ref(slot, stage):
        if stage < ROW_CUTS:
            return w_gu.at[slot, pl.ds(stage * depth, depth)]
        return w_d.at[slot, :, pl.ds(*spans[stage - ROW_CUTS])]

    def weight_all(slot, down):
        return (w_d if down else w_gu).at[slot]

    def weight_out(piece, step):
        kind, part_id = pieces[piece]
        stage = ROW_CUTS + part_id if kind == 2 else part_id
        return remote(
            weight_src(piece), weight_dst(tp, piece),
            out_send.at[kind // 2, step - 1], far_recv.at[stage, step - 1],
            (sp, lax.rem(yi + step, pairs) * 2 + half_c),
        )

    def pair_slot(step):
        return lax.rem(yi + step, pairs) * 2 + half_c

    def far_arrival(stage, step):
        block = stage_ref(pair_slot(step), stage)
        return remote(
            block, block, out_send.at[0, 0], far_recv.at[stage, pairs - step - 1], (sp, mate)
        )

    def stage_mate(stage, step):
        block = stage_ref(pair_slot(step), stage)
        return remote(
            block, block, relay_send.at[int(stage >= ROW_CUTS), step - 1],
            relay_recv.at[stage, step - 1], (sp, mate),
        )

    def relay_arrival(stage, step):
        block = stage_ref(lax.rem(yi + step, pairs) * 2 + 1 - half_c, stage)
        return remote(
            block, block, relay_send.at[0, 0], relay_recv.at[stage, step - 1], (sp, mate)
        )

    def relay(stage):
        for step in range(1, pairs):
            far_arrival(stage, step).wait_recv()
            stage_mate(stage, step).start()

    def from_mate(stage):
        for step in range(1, pairs):
            relay_arrival(stage, step).wait_recv()

    own_weights = [
        (rg_hbm, w_gu.at[tp, :, pl.ds(0, fe)], 0),
        (ru_hbm, w_gu.at[tp, :, pl.ds(fe, fe)], 0),
        (rd_hbm, w_d.at[tp], 1),
    ]
    halo_copy = remote(
        rec_in.at[pl.ds(length - 8, 8)], halo, halo_sem.at[0], halo_sem.at[1],
        (lax.rem(sp + 1, sp_n), tp),
    )
    pl.semaphore_wait(barrier, sp_n - 1 + tp_n - 1)
    order = [0, gate_pieces, *range(1, gate_pieces), *range(gate_pieces + 1, len(pieces))]

    def send_weights(piece):
        for step in range(1, pairs):
            weight_out(piece, step).start()

    for place, least in enumerate(EARLY):
        pl.when(sp >= least)(functools.partial(send_weights, order[place]))
    loads[0].wait()

    @pl.when(sp + 1 < sp_n)
    def _():
        halo_copy.start()

    out_w_load = pltpu.make_async_copy(out_w_hbm, out_w, local_sem.at[0])
    out_w_load.start()
    for src, dst, down in own_weights:
        remote(src, dst, own_send.at[down], own_recv.at[down], (sp, mate)).start()
        pltpu.make_async_copy(src, dst, local_sem.at[1 + down]).start()
    shared_loads = [
        pltpu.make_async_copy(sg_hbm, s_gu.at[:, pl.ds(0, fs)], local_sem.at[3]),
        pltpu.make_async_copy(su_hbm, s_gu.at[:, pl.ds(fs, fs)], local_sem.at[4]),
        pltpu.make_async_copy(sd_hbm, s_d, local_sem.at[5]),
    ]
    for load in shared_loads:
        load.start()
    for load in loads[1:]:
        load.wait()

    expert = lax.broadcasted_iota(jnp.int32, (wdense.shape[0], length), 0)
    table = jnp.zeros((wdense.shape[0], length), F32)
    for k in range(ids.shape[0]):
        table = table + jnp.where(expert == ids[k : k + 1], wts[k : k + 1], 0.0)
    wdense[...] = table
    w_in[sp] = table

    def w_out(step):
        return remote(
            wdense, w_in.at[sp], w_send.at[0], w_recv.at[0], (lax.rem(sp + step, sp_n), tp)
        )

    small_blocks, large_blocks = lane_blocks(small_maps), lane_blocks(large_maps)
    rate_rows = -8.0 * softplus(-channel_decay[...])
    rate = jnp.concatenate([rate_rows[0:1], rate_rows[1:2]], axis=1)
    tap_rows = [
        jnp.concatenate([taps[k, 0:1], taps[k, 1:2]], axis=1).astype(F32)
        for k in range(taps.shape[0])
    ]

    padded[pl.ds(8, length)] = rec_in[...].astype(F32).reshape(length, chans)
    tap_n = taps.shape[0]

    def segment(first, count):
        base = 8 + first - tap_n + 1
        summed = tap_rows[0] * padded[pl.ds(base, count)]
        for k in range(1, tap_n):
            summed = summed + tap_rows[k] * padded[pl.ds(base + k, count)]
        conv = summed.astype(BF16)
        outs = [
            dot(conv[:, i * LANES : (i + 1) * LANES], maps)
            for i, maps in enumerate(small_blocks + large_blocks)
        ]
        recur = jax.nn.sigmoid(jnp.concatenate([o[:, :LANES] for o in outs], axis=1))
        inp = jax.nn.sigmoid(jnp.concatenate([o[:, LANES:] for o in outs], axis=1))
        log_decay = recur * rate + extra[pl.ds(first, count)].reshape(count, chans)
        decay = jnp.exp(log_decay)
        state = jnp.sqrt(-expm1_negative(2.0 * log_decay)) * inp * conv.astype(F32)
        row_id = lax.broadcasted_iota(jnp.int32, (count, chans), 0)
        shift = 1
        while shift < count:
            live = row_id >= shift
            before_a = jnp.where(live, pltpu.roll(decay, shift, 0), 1.0)
            before_b = jnp.where(live, pltpu.roll(state, shift, 0), 0.0)
            state = decay * before_b + state
            decay = decay * before_a
            shift *= 2
        return decay, state

    decay_b, state_b = segment(8, length - 8)
    scan_a[...] = decay_b
    scan_b[...] = state_b

    @pl.when(sp == 0)
    def _():
        padded[pl.ds(0, 8)] = jnp.zeros((8, chans), F32)

    @pl.when(sp > 0)
    def _():
        halo_copy.wait_recv()
        padded[pl.ds(0, 8)] = halo[...].astype(F32).reshape(8, chans)

    decay_a, state_a = segment(0, 8)
    end_a, end_b = scan_a[length - 9 :], scan_b[length - 9 :]
    carry_own[...] = jnp.concatenate(
        [end_a * decay_a[7:], end_a * state_a[7:] + end_b], axis=0
    )

    def carry_out(step):
        return remote(
            carry_own, carry_in.at[sp], carry_send.at[step], carry_recv.at[sp],
            (lax.rem(sp + step, sp_n), tp),
        )

    def carry_arrival(who):
        return remote(
            carry_own, carry_in.at[who], carry_send.at[0], carry_recv.at[who], (sp, tp)
        )

    @pl.loop(1, sp_n)
    def _(back):
        step = sp_n - back

        @pl.when(sp + step < sp_n)
        def _():
            carry_out(step).start()

    @pl.loop(1, sp_n)
    def _(step):
        w_out(step).start()

    gi = gate_in[...].astype(F32).reshape(length, chans)
    gelu = 0.5 * gi * (1.0 + jnp.tanh(0.7978845608028654 * (gi + 0.044715 * gi * gi * gi)))

    def fold(who, incoming):
        carry_arrival(who).wait_recv()
        link = carry_in[who]
        return link[0:1] * incoming + link[1:2]

    incoming = lax.fori_loop(0, sp, fold, jnp.zeros((1, chans), F32))
    head = state_a + decay_a * incoming
    rest = scan_b[...] + scan_a[...] * head[7:]
    branch = (gelu * jnp.concatenate([head, rest], axis=0)).astype(BF16)
    out_w_load.wait()
    part[...] = dot(branch, out_w[...]).astype(BF16).reshape(part.shape)

    def pair_copy(step):
        slot = lax.rem(yi + step, pairs) * 2 + 1 - half_c
        return remote(
            part.at[slot], pair_in.at[step], pair_send.at[0], pair_recv.at[step], (sp, mate)
        )

    def part_out(step):
        to = lax.rem(yi + step, pairs)
        return remote(
            pair_out.at[step], part_in.at[yi], tp_send.at[step - 1], tp_recv.at[step - 1],
            (sp, to * 2 + half_c),
        )

    def part_arrival(step):
        who = lax.rem(yi + step, pairs)
        return remote(
            pair_out.at[0], part_in.at[who], tp_send.at[0], tp_recv.at[pairs - step - 1], (sp, mate)
        )

    for step in range(1, pairs + 1):
        pair_copy(step % pairs).start()
    for step in range(1, pairs):
        pair_copy(step).wait_recv()
        pair_out[step] = (
            part[pair_slot(step)].astype(F32) + pair_in[step].astype(F32)
        ).astype(BF16)
        part_out(step).start()
    for place, least in enumerate(EARLY):
        if least:
            pl.when(sp < least)(functools.partial(send_weights, order[place]))
    for piece in order[len(EARLY) :]:
        send_weights(piece)
    @pl.loop(1, sp_n)
    def _(step):
        @pl.when(sp + step < sp_n)
        def _():
            carry_out(step).wait_send()

    pair_copy(0).wait_recv()
    mixed = part[tp].astype(F32) + pair_in[0].astype(F32)
    for step in range(1, pairs):
        who = lax.rem(yi + step, pairs)
        part_arrival(step).wait_recv()
        mixed = mixed + part_in[who].astype(F32)
    normed = layer_norm(
        RESIDUAL_SCALE * stream[...].astype(F32) + mixed, n1g[...], n1b[...]
    ).astype(BF16)
    rows[xi, zi] = normed

    def row_piece(col, zj, h):
        return rows.at[col, zj, :, pl.ds(h * half_w, half_w)]

    def row_copy(zj, h, sems, where):
        piece = row_piece(xi, zj, h)
        return remote(piece, piece, sems, ag_recv.at[zj, h], (where, tp))

    def row_right(zj, h):
        return row_copy(zj, h, right_send.at[zj], (zi + 1) * inner + xi)

    def row_left(zj, h):
        return row_copy(zj, h, left_send.at[zj], (zi - 1) * inner + xi)

    def row_across(zj, h):
        piece = row_piece(xi, zj, h)
        return remote(piece, piece, fw_send.at[0], agx_recv.at[0], (x_peer, tp))

    def row_arrival(zj, h):
        piece = row_piece(xi, zj, h)
        return remote(piece, piece, fw_send.at[0], ag_recv.at[zj, h], (x_peer, tp))

    last = outer - 1

    def goes_right(zj):
        far = jnp.logical_and(zj == 0, zi == last - 1)
        return jnp.logical_and(zi < last, jnp.logical_not(far) if outer > 2 else True)

    def goes_left(zj):
        far = jnp.logical_and(zj == last, zi == 1)
        return jnp.logical_and(zi > 0, jnp.logical_not(far) if outer > 2 else True)

    for h in range(SPLITS):
        @pl.when(zi < last)
        def _():
            row_right(zi, h).start()

        @pl.when(zi > 0)
        def _():
            row_left(zi, h).start()

        row_across(zi, h).start()

    if outer > 2:
        for h in range(SPLITS):
            @pl.when(zi == 0)
            def _():
                row_copy(zi, h, left_send.at[zi], last * inner + xi).start()

            @pl.when(zi == last)
            def _():
                row_copy(zi, h, right_send.at[zi], xi).start()

    for stage in (0, ROW_CUTS):
        relay(stage)

    def pass_on(step):
        for h in range(SPLITS):
            @pl.when(zi - step >= 0)
            def _():
                row_arrival(zi - step, h).wait_recv()

                @pl.when(goes_right(zi - step))
                def _():
                    row_right(zi - step, h).start()

                row_across(zi - step, h).start()

            @pl.when(zi + step < outer)
            def _():
                row_arrival(zi + step, h).wait_recv()

                @pl.when(goes_left(zi + step))
                def _():
                    row_left(zi + step, h).start()

                row_across(zi + step, h).start()

    for stage in range(1, ROW_CUTS - 1):
        if stage < outer:
            pass_on(stage)
        relay(stage)

    @pl.loop(ROW_CUTS - 1, outer)
    def _(step):
        pass_on(step)

    for load in shared_loads:
        load.wait()
    up = dot(normed, s_gu[...])
    s_hid = (silu(up[:, :fs]) * up[:, fs:]).astype(BF16)
    moe[...] = dot(s_hid, s_d[...]) + RESIDUAL_SCALE * normed.astype(F32)

    tables = w_in.at[pl.ds(0, sp_n - 1)]
    remote(tables, tables, w_send.at[0], w_recv.at[0], (x_peer, tp)).wait_recv()

    own_rows = lax.broadcasted_iota(jnp.int32, (quarter, length), 0) + tp * quarter
    pick = lax.broadcasted_iota(jnp.int32, (quarter, length), 1) == own_rows

    batch = min(outer, 4)
    tall = batch * quarter
    cap = hid_pack.shape[1] // batch

    def token_weights(col, zj, expert_id):
        line = w_in[zj * inner + col, pl.ds(expert_id, 1)]
        weight = jnp.sum(jnp.where(pick, line, 0.0), axis=1, keepdims=True)
        return jnp.broadcast_to(weight, (quarter, LANES))

    @pl.loop(0, outer)
    def _(zj):
        for j in range(inner):
            w_rows[j, zj] = token_weights(j, zj, sp)
        w_peer[zj] = token_weights(xi, zj, x_peer)

    t_row = lax.broadcasted_iota(jnp.int32, (tall, tall), 0)
    t_col = lax.broadcasted_iota(jnp.int32, (tall, tall), 1)
    same = t_row // quarter == t_col // quarter
    earlier = jnp.where(jnp.logical_and(same, t_col < t_row), 1.0, 0.0).astype(BF16)
    slot_base = (t_row // quarter * cap).astype(F32)

    def places(weights):
        chosen = weights > 0.0
        rank = dot(earlier, jnp.where(chosen, 1.0, 0.0).astype(BF16))
        hit = jnp.logical_and(chosen, t_col.astype(F32) == rank + slot_base)
        return jnp.where(hit, 1.0, 0.0).astype(BF16)

    @pl.loop(0, outer // batch)
    def _(i):
        group = pl.ds(i * batch, batch)
        place_out[i] = places(w_rows[other_x, group].reshape(tall, LANES))
        place_in[i] = places(w_peer[group].reshape(tall, LANES))

    for down in (0, 1):
        own = weight_all(tp, down)
        pltpu.make_async_copy(own, own, local_sem.at[1 + down]).wait()
        theirs = weight_all(mate, down)
        remote(theirs, theirs, own_send.at[down], own_recv.at[down], (sp, mate)).wait_recv()

    def gate_up(col, stage):
        final = stage == ROW_CUTS - 1

        @pl.loop(0, outer // batch)
        def _(i):
            block = rows[
                col, pl.ds(i * batch, batch), :, stage * depth : (stage + 1) * depth
            ].reshape(tall, depth)
            for t in range(tp_n):
                gu = dot(block, w_gu[t, stage * depth : (stage + 1) * depth])
                if stage:
                    gu = gu + gu_acc[col, i, :, t * 2 * fe : (t + 1) * 2 * fe]
                if final:
                    act = (silu(gu[:, :fe]) * gu[:, fe:]).astype(BF16)
                    hid[col, i, :, t * fe : (t + 1) * fe] = act
                else:
                    gu_acc[col, i, :, t * 2 * fe : (t + 1) * 2 * fe] = gu

    for stage in range(ROW_CUTS - 1):
        from_mate(stage)
        gate_up(xi, stage)
    relay(ROW_CUTS - 1)
    side = rows.at[other_x]
    remote(side, side, fw_send.at[0], agx_recv.at[0], (x_peer, tp)).wait_recv()
    for stage in range(ROW_CUTS - 1):
        gate_up(other_x, stage)
    from_mate(ROW_CUTS - 1)
    gate_up(other_x, ROW_CUTS - 1)

    @pl.loop(0, outer // batch)
    def _(i):
        packed = lax.dot_general(
            place_out[i], hid[other_x, i], (((0,), (0,)), ((), ())), preferred_element_type=F32
        )
        hid_pack[i] = packed[: batch * cap].astype(BF16)

    gate_up(xi, ROW_CUTS - 1)

    def columns(ref, c):
        return ref.at[:, :, pl.ds(*spans[c])]

    def x_out(c):
        return remote(
            columns(y_out, c), columns(x_in, c), xs_send.at[0], xs_recv.at[c], (x_peer, tp)
        )

    def z_target(step):
        down_to, up_to = last + 1 - step, step - 1
        down_to = jnp.where(down_to > zi, down_to, down_to - 1)
        up_to = jnp.where(up_to < zi, up_to, up_to + 1)
        return jnp.where(zi < outer // 2, down_to, up_to)

    def z_send(c, step):
        zj = z_target(step)
        return remote(
            columns(z_out, c).at[zj], columns(z_in, c).at[zi], zs_send.at[0], zs_recv.at[c],
            (zj * inner + xi, tp),
        )

    def down_across(c):
        first, wide = spans[c]

        @pl.loop(0, outer // batch)
        def _(i):
            value = dot(
                hid_pack[i], w_d[:, :, first : first + wide].reshape(tp_n * fe, wide)
            )
            y_out[i, :, first : first + wide] = value.astype(BF16)

    def down_own(c):
        first, wide = spans[c]

        @pl.loop(0, outer // batch)
        def _(i):
            value = dot(
                hid[xi, i], w_d[:, :, first : first + wide].reshape(tp_n * fe, wide)
            )
            weight = w_rows[xi, pl.ds(i * batch, batch)].reshape(tall, LANES)
            for a in range(0, wide, LANES):
                y_own[pl.ds(i * batch, batch), :, first + a : first + a + LANES] = (
                    (weight * value[:, a : a + LANES]).reshape(batch, quarter, LANES)
                )

    def merge(c):
        first, wide = spans[c]
        at = slice(first, first + wide)
        x_out(c).wait_recv()

        @pl.loop(0, outer // batch)
        def _(i):
            group = pl.ds(i * batch, batch)
            value = dot(place_in[i][:, : batch * cap], x_in[i, :, at])
            weight = w_peer[group].reshape(tall, LANES)
            for a in range(0, wide, LANES):
                cols = slice(first + a, first + a + LANES)
                z_out[group, :, cols] = (
                    y_own[group, :, cols]
                    + (weight * value[:, a : a + LANES]).reshape(batch, quarter, LANES)
                ).astype(BF16)

        @pl.loop(1, outer)
        def _(step):
            z_send(c, step).start()

        moe[:, at] = moe[:, at] + z_out[zi, :, at].astype(F32)

    chunks = len(spans)
    for c in range(chunks):
        from_mate(ROW_CUTS + c)
        down_across(c)
        x_out(c).start()
        if c + 1 < chunks:
            relay(ROW_CUTS + c + 1)
        down_own(c)
        if c >= 2:
            merge(c - 2)
    merge(chunks - 2)
    merge(chunks - 1)

    for c in range(chunks):
        first, wide = spans[c]
        at = slice(first, first + wide)
        group = columns(z_in, c).at[pl.ds(0, outer - 1)]
        remote(group, group, zs_send.at[0], zs_recv.at[c], (x_peer, tp)).wait_recv()

        @pl.loop(1, outer)
        def _(step):
            moe[:, at] += z_in[lax.rem(zi + step, outer), :, at].astype(F32)

    result[...] = layer_norm(moe[...], n2g[...], n2b[...]).astype(BF16)

    for down in (0, 1):
        whole = weight_all(tp, down)
        for step in range(1, pairs):
            remote(whole, whole, out_send.at[down, step - 1], own_recv.at[0], (sp, mate)).wait_send()
            remote(
                whole, whole, relay_send.at[down, step - 1], own_recv.at[0], (sp, mate)
            ).wait_send()
        remote(whole, whole, own_send.at[down], own_recv.at[0], (sp, mate)).wait_send()
    remote(pair_in, pair_in, pair_send.at[0], pair_recv.at[0], (sp, mate)).wait_send()
    for step in range(1, pairs):
        part_out(step).wait_send()
    remote(tables, tables, w_send.at[0], w_recv.at[0], (x_peer, tp)).wait_send()

    @pl.when(sp + 1 < sp_n)
    def _():
        halo_copy.wait_send()

    @pl.loop(0, outer)
    def _(zj):
        block = rows.at[xi, zj]

        ends = jnp.logical_and(zj == zi, outer > 2)

        @pl.when(
            jnp.logical_or(
                jnp.logical_and(zj <= zi, goes_right(zj)), jnp.logical_and(ends, zi == last)
            )
        )
        def _():
            remote(block, block, right_send.at[zj], fw_send.at[0], (x_peer, tp)).wait_send()

        @pl.when(
            jnp.logical_or(
                jnp.logical_and(zj >= zi, goes_left(zj)), jnp.logical_and(ends, zi == 0)
            )
        )
        def _():
            remote(block, block, left_send.at[zj], fw_send.at[0], (x_peer, tp)).wait_send()

    remote(side, side, fw_send.at[0], agx_recv.at[0], (x_peer, tp)).wait_send()
    remote(y_out, y_out, xs_send.at[0], agx_recv.at[0], (x_peer, tp)).wait_send()
    sent = z_out.at[pl.ds(0, outer - 1)]
    remote(sent, sent, zs_send.at[0], agx_recv.at[0], (x_peer, tp)).wait_send()


def shards(
    dims,
    stream,
    recurrence_input,
    output_gate_input,
    convolution_taps,
    first_group_gates,
    second_group_gates,
    channel_decay,
    position_log_extra,
    recurrence_output_weight,
    first_norm_gain,
    first_norm_bias,
    routed_expert_index,
    routed_expert_weight,
    routed_gate_weight,
    routed_up_weight,
    routed_down_weight,
    shared_gate_weight,
    shared_up_weight,
    shared_down_weight,
    second_norm_gain,
    second_norm_bias,
):
    sp_n, tp_n, inner = dims
    outer = sp_n // inner
    length = recurrence_input.shape[0]
    chans = 2 * recurrence_input.shape[2]
    quarter, width = stream.shape
    fe = routed_gate_weight.shape[2]
    fs = shared_gate_weight.shape[1]
    vec = lambda a: a.reshape(1, width)
    vmem = pl.BlockSpec(memory_space=pltpu.VMEM)
    hbm = pl.BlockSpec(memory_space=pltpu.HBM)
    dma = pltpu.SemaphoreType.DMA
    block = (quarter, width)
    pairs = tp_n // 2
    stages = ROW_CUTS + len(COLUMN_CUTS)
    batch = min(outer, 4)
    tall = batch * quarter
    cap = 5 * quarter * routed_expert_index.shape[1] // (4 * sp_n)
    operands = (
        stream,
        recurrence_input,
        output_gate_input,
        convolution_taps,
        first_group_gates,
        second_group_gates,
        channel_decay,
        position_log_extra,
        vec(first_norm_gain),
        vec(first_norm_bias),
        vec(second_norm_gain),
        vec(second_norm_bias),
        routed_expert_index.T,
        routed_expert_weight.T,
    )
    weights = (
        recurrence_output_weight.reshape(chans, width),
        routed_gate_weight.reshape(width, fe),
        routed_up_weight.reshape(width, fe),
        routed_down_weight.reshape(fe, width),
        shared_gate_weight,
        shared_up_weight,
        shared_down_weight,
    )
    limit = (28 + sp_n // 2) * 2**20
    operands = tuple(pltpu.with_memory_space_constraint(a, pltpu.HBM) for a in operands)
    weights = tuple(pltpu.with_memory_space_constraint(a, pltpu.HBM) for a in weights)
    return pl.pallas_call(
        functools.partial(kernel, dims),
        out_shape=jax.ShapeDtypeStruct(block, BF16),
        in_specs=[hbm] * (len(operands) + len(weights)),
        out_specs=vmem,
        scratch_shapes=[
            *(pltpu.VMEM(a.shape, a.dtype) for a in operands),
            dma((len(operands),)),
            pltpu.VMEM((length + 8, chans), F32),
            pltpu.VMEM((8,) + recurrence_input.shape[1:], BF16),
            pltpu.VMEM((length - 8, chans), F32),
            pltpu.VMEM((length - 8, chans), F32),
            pltpu.VMEM((2, chans), F32),
            pltpu.VMEM((sp_n, 2, chans), F32),
            pltpu.VMEM((sp_n, length), F32),
            pltpu.VMEM((sp_n, sp_n, length), F32),
            pltpu.VMEM((inner, outer, quarter, LANES), F32),
            pltpu.VMEM((outer, quarter, LANES), F32),
            pltpu.VMEM((outer // batch, tall, LANES), BF16),
            pltpu.VMEM((outer // batch, tall, LANES), BF16),
            pltpu.VMEM((chans, width), BF16),
            pltpu.VMEM((tp_n, width, 2 * fe), BF16),
            pltpu.VMEM((tp_n, fe, width), BF16),
            pltpu.VMEM((width, 2 * fs), BF16),
            pltpu.VMEM((fs, width), BF16),
            pltpu.VMEM((tp_n,) + block, BF16),
            pltpu.VMEM((pairs,) + block, BF16),
            pltpu.VMEM((pairs,) + block, BF16),
            pltpu.VMEM((pairs,) + block, BF16),
            pltpu.VMEM((inner, outer) + block, BF16),
            pltpu.VMEM((inner, outer // batch, tall, tp_n * fe), BF16),
            pltpu.VMEM((outer // batch, batch * cap, tp_n * fe), BF16),
            pltpu.VMEM((inner, outer // batch, batch * quarter, tp_n * 2 * fe), F32),
            pltpu.VMEM((outer,) + block, F32),
            pltpu.VMEM((outer // batch, batch * cap, width), BF16),
            pltpu.VMEM((outer // batch, batch * cap, width), BF16),
            pltpu.VMEM((outer,) + block, BF16),
            pltpu.VMEM((outer,) + block, BF16),
            pltpu.VMEM(block, F32),
            dma((6,)),
            dma((2,)),
            dma((sp_n,)),
            dma((sp_n,)),
            dma((1,)),
            dma((1,)),
            dma((2, pairs - 1)),
            dma((2,)),
            dma((2, pairs - 1)),
            dma((2,)),
            dma((stages, pairs - 1)),
            dma((stages, pairs - 1)),
            dma((1,)),
            dma((pairs,)),
            dma((pairs - 1,)),
            dma((pairs - 1,)),
            dma((1,)),
            dma((outer, SPLITS)),
            dma((1,)),
            dma((1,)),
            dma((1,)),
        ],
        compiler_params=pltpu.CompilerParams(
            has_side_effects=True, collective_id=0, vmem_limit_bytes=limit
        ),
    )(*operands, *weights)


def solution(mesh):
    in_specs = (
        P(("sp", "tp"), None),
        P("sp", None, "tp"),
        P("sp", None, "tp"),
        P(None, None, "tp"),
        P(None, "tp", None, None),
        P(None, "tp", None, None),
        P(None, "tp"),
        P("sp", None, "tp"),
        P(None, "tp", None),
        P(),
        P(),
        P("sp", None),
        P("sp", None),
        P("sp", None, "tp"),
        P("sp", None, "tp"),
        P("sp", "tp", None),
        P(),
        P(),
        P(),
        P(),
        P(),
    )
    dims = (mesh.shape["sp"], mesh.shape["tp"], 2)
    return jax.shard_map(
        functools.partial(shards, dims),
        mesh=mesh,
        in_specs=in_specs,
        out_specs=P(("sp", "tp"), None),
        check_vma=False,
    )
```
